1024 devices in a mesh: sp: 32 (over z), tp: 4 (over y), dp: 8 (over x, core).
Axes of the slice: x: 4, y: 4, z: 32, core: 2. Of those that a mesh axis runs over, the one named last changes fastest.
Arguments:
- latent: bfloat16 [32768, 2048], P(('dp', 'sp', 'tp')), parts along dimension 0, may hold values from -6 to 6
- cond: bfloat16 [16384], P('dp'), parts along dimension 0, may hold values from -6 to 6
- context: bfloat16 [4096, 2048], P(('dp', 'sp')), parts along dimension 0, may hold values from -6 to 6
- context_cond: bfloat16 [2048], replicated, may hold values from -6 to 6
- modulation: bfloat16 [2048, 6144], P(('sp', 'tp')), may hold values from -0.125 to 0.125
- norm_gain: bfloat16 [2048], replicated, may hold values from 0.099609375 to 1.8984375
- w_x: bfloat16 [2048, 1024], P(None, 'tp'), may hold values from -0.125 to 0.125
- w_gate: bfloat16 [2048, 1024], P(None, 'tp'), may hold values from -0.125 to 0.125
- w_b: bfloat16 [2048, 256], P(None, 'tp'), may hold values from -0.125 to 0.125
- w_c: bfloat16 [2048, 256], P(None, 'tp'), may hold values from -0.125 to 0.125
- w_dt: bfloat16 [2, 2048, 16], P(None, None, 'tp'), may hold values from -0.125 to 0.125
- conv_x: bfloat16 [4, 1024], P(None, 'tp'), may hold values from -3 to 3
- conv_b: bfloat16 [4, 256], P(None, 'tp'), may hold values from -3 to 3
- conv_c: bfloat16 [4, 256], P(None, 'tp'), may hold values from -3 to 3
- decay_rate: float32 [2, 16], P(None, 'tp'), may hold values from 0 to 0.04
- decay_extra: float32 [32768, 16], P(('dp', 'sp'), 'tp'), parts along dimension 0, may hold values from -2 to 0
- out_gain: bfloat16 [1024], P('tp'), may hold values from 0.099609375 to 1.8984375
- w_out: bfloat16 [1024, 2048], replicated, may hold values from -0.1875 to 0.1875
Outputs:
- mixed: bfloat16 [32768, 2048], P(('dp', 'sp', 'tp')), parts along dimension 0
The draws below stay inside these ranges and needn't reach their ends.
There are 8 independent parts, one for each index of `dp`. The reference program is written for one: setup_inputs(seed, part) draws one part's arguments, and reference() takes and returns one part's arrays. A program takes and returns all parts, laid end to end along the dimension named above; an argument that names none is the same for every part. Nothing has to cross between parts.
All inputs are finite; a program needn't handle non-finite values.
Results may differ from the reference program's by a relative error of at most 0.007.
Values may be sent and summed in bfloat16 or wider, within the bound.
No kernel may reach another device: no remote copies, remote signals or barrier semaphores. Data moves between devices by JAX's collectives and lax.ppermute only.
A program may use at most 64 MiB of HBM per device.

```python
import math
import jax
import jax.numpy as jnp
from jax import lax

D = 2048
MIXER_HEADS = 16
HEAD_DIM = 64
GROUPS = 4
STATE = 64
TAPS = 4
BLOCK = 128
TOK_DEV = 128
CTX = 512
LATENT_TOKENS = 4096


def draw_decay_rate(key, part):
    pick_key, fast_key, slow_key = jax.random.split(key, 3)
    fast_share = 0.5
    chosen = jax.random.uniform(pick_key, (2, MIXER_HEADS), jnp.float32) < fast_share
    fast_rate = jnp.exp(jax.random.uniform(fast_key, (2, MIXER_HEADS), jnp.float32, math.log(0.015), math.log(0.04)))
    slow_rate = jnp.exp(jax.random.uniform(slow_key, (2, MIXER_HEADS), jnp.float32, math.log(0.2), 0.0)) / LATENT_TOKENS
    return jnp.where(chosen, fast_rate, slow_rate)


def draw_decay_extra(key, part):
    block_key, head_key, position_random_key, depth_random_key = jax.random.split(key, 4)
    blocks = LATENT_TOKENS // TOK_DEV
    factor = jnp.exp(jax.random.uniform(block_key, (blocks, 1), jnp.float32, 0.0, math.log(8.0)))
    head_scale = jax.random.uniform(head_key, (1, MIXER_HEADS), jnp.float32, 0.5, 1.5)
    steady_portion = jnp.repeat(-(0.2 / LATENT_TOKENS) * factor * head_scale, TOK_DEV, axis=0)
    spike_positions = jax.random.randint(position_random_key, (2,), 0, LATENT_TOKENS)
    spike_depth = jnp.log(jax.random.uniform(depth_random_key, (2, MIXER_HEADS), jnp.float32, 0.5, 0.8))
    spike_rows = (jnp.arange(LATENT_TOKENS)[:, None] == spike_positions[None, :]).astype(jnp.float32)
    return steady_portion + jnp.dot(spike_rows, spike_depth)


def block_scale(rng, extent, pieces, least, largest):
    level, own = 1.0, jax.random.fold_in(rng, 6)
    for position, shards_of in pieces:
        heights = jnp.exp(jax.random.uniform(jax.random.fold_in(own, position), (shards_of,), jnp.float32, least / len(pieces), largest / len(pieces)))
        level = level * jnp.repeat(heights, extent[position] // shards_of).reshape([-1 if axis == position else 1 for axis in range(len(extent))])
    return level


def gaussian(own_key, extent, deviation, reach, cuts=(), held_as=jnp.bfloat16):
    drawn = jax.random.normal(own_key, extent, jnp.float32) * deviation
    if len(cuts) > 0:
        drawn = block_scale(own_key, extent, cuts, -0.22, 0.18) * drawn
    return jnp.clip(drawn, min=-reach, max=reach).astype(held_as)


def setup_inputs(seed: int = 0, part: int = 0) -> dict:
    seeds = jax.random.split(jax.random.key(seed), 19)
    own_keys = jax.random.split(jax.random.fold_in(seeds[18], part), 19)
    return {
        "latent": gaussian(own_keys[0], (LATENT_TOKENS, D), 1.0, 6.0, ((0, 128),)),
        "cond": gaussian(own_keys[1], (D,), 1.0, 6.0),
        "context": gaussian(own_keys[2], (CTX, D), 1.0, 6.0, ((0, 32),)),
        "context_cond": gaussian(seeds[3], (D,), 1.0, 6.0),
        "modulation": gaussian(seeds[4], (D, 3 * D), D ** -0.5, 0.125, ((0, 128),)),
        "norm_gain": jnp.clip(1.0 + 0.18 * jax.random.normal(seeds[5], (D,), jnp.float32), 0.099609375, 1.8984375).astype(jnp.bfloat16),
        "w_x": gaussian(seeds[6], (D, MIXER_HEADS * HEAD_DIM), D ** -0.5, 0.125, ((1, 4),)),
        "w_gate": gaussian(seeds[7], (D, MIXER_HEADS * HEAD_DIM), D ** -0.5, 0.125, ((1, 4),)),
        "w_b": gaussian(seeds[8], (D, GROUPS * STATE), D ** -0.5, 0.125, ((1, 4),)),
        "w_c": gaussian(seeds[9], (D, GROUPS * STATE), D ** -0.5, 0.125, ((1, 4),)),
        "w_dt": gaussian(seeds[10], (2, D, MIXER_HEADS), D ** -0.5, 0.125, ((2, 4),)),
        "conv_x": gaussian(seeds[11], (TAPS, MIXER_HEADS * HEAD_DIM), TAPS ** -0.5, 3.0, ((1, 4),)),
        "conv_b": gaussian(seeds[12], (TAPS, GROUPS * STATE), TAPS ** -0.5, 3.0, ((1, 4),)),
        "conv_c": gaussian(seeds[13], (TAPS, GROUPS * STATE), TAPS ** -0.5, 3.0, ((1, 4),)),
        "decay_rate": draw_decay_rate(jax.random.fold_in(seeds[18], 71), part),
        "decay_extra": draw_decay_extra(jax.random.fold_in(jax.random.fold_in(seeds[18], part), 71), part),
        "out_gain": jnp.clip(1.0 + 0.18 * jax.random.normal(seeds[16], (MIXER_HEADS * HEAD_DIM,), jnp.float32), 0.099609375, 1.8984375).astype(jnp.bfloat16),
        "w_out": gaussian(seeds[17], (MIXER_HEADS * HEAD_DIM, D), (MIXER_HEADS * HEAD_DIM) ** -0.5, 0.1875),
    }


ROW_EPS = 1e-06
GROUP_EPS = 1e-05
HIGHEST = lax.Precision.HIGHEST

def modulated_norm(row_block, norm_gain, shift_row, scale_row):
    values = row_block.astype(jnp.float32)
    normed = values * lax.rsqrt(lax.optimization_barrier(jnp.mean(values * values, axis=-1, keepdims=True)) + ROW_EPS)
    return (normed * norm_gain.astype(jnp.float32) * (1.0 + scale_row) + shift_row).astype(jnp.bfloat16)

def project(row_block, weight):
    return jnp.dot(row_block, weight, preferred_element_type=jnp.float32).astype(jnp.bfloat16)

def conv_padded(padded, conv_taps, length):
    values = padded.astype(jnp.float32)
    summed = jnp.zeros((length, values.shape[1]), jnp.float32)
    for offset in range(conv_taps.shape[0]):
        summed = summed + conv_taps[offset].astype(jnp.float32) * values[offset:offset + length]
    return jax.nn.silu(summed).astype(jnp.bfloat16)

def short_conv(projected, conv_taps):
    padded = jnp.pad(projected, ((2, 1), (0, 0)))
    return conv_padded(padded, conv_taps, projected.shape[0])

def context_states(ctx_xs, ctx_bmat, ctx_dt, decay_rate):
    length = ctx_xs.shape[0]
    groups = ctx_bmat.shape[1] // STATE
    heads_here = ctx_dt.shape[2]
    repeat = heads_here // groups
    values = ctx_xs.astype(jnp.float32).reshape(length, groups, repeat, HEAD_DIM)
    keys_b = ctx_bmat.astype(jnp.float32).reshape(length, groups, STATE)
    log_decay = -decay_rate[:, None, :] * ctx_dt
    running = jnp.cumsum(log_decay, axis=1)
    forward_weight = (jnp.exp(running[0, -1:] - running[0]) * ctx_dt[0]).reshape(length, groups, repeat)
    backward_weight = (jnp.exp(running[1] - log_decay[1]) * ctx_dt[1]).reshape(length, groups, repeat)
    forward_state = jnp.einsum('lgn,lgr,lgrp->grpn', keys_b, forward_weight, values, precision=HIGHEST)
    backward_state = jnp.einsum('lgn,lgr,lgrp->grpn', keys_b, backward_weight, values, precision=HIGHEST)
    return (forward_state, backward_state)

def to_bf16_and_back(values):
    rounded = values.astype(jnp.bfloat16)
    rounded = lax.optimization_barrier(rounded)
    return rounded.astype(jnp.float32)

def block_pass(inputs, step_sizes, log_decay, bmat, cmat, start_state):
    length = inputs.shape[0]
    groups, repeat = (start_state.shape[0], start_state.shape[1])
    block_count = length // BLOCK
    values = inputs.reshape(block_count, BLOCK, groups, repeat, HEAD_DIM)
    steps_blk = step_sizes.reshape(block_count, BLOCK, groups, repeat)
    decays = log_decay.reshape(block_count, BLOCK, groups, repeat)
    keys_b = bmat.reshape(block_count, BLOCK, groups, STATE)
    reads_c = cmat.reshape(block_count, BLOCK, groups, STATE)
    lower_mask = (jnp.arange(BLOCK)[:, None] >= jnp.arange(BLOCK)[None, :])[:, :, None, None]

    def advance(carried, block_data):
        value_blk, step_blk, decay_blk, key_blk, read_blk = block_data
        value_f = value_blk.astype(jnp.float32)
        key_f = key_blk.astype(jnp.float32)
        read_f = read_blk.astype(jnp.float32)
        running = jnp.cumsum(decay_blk, axis=0)
        log_gaps = running[:, None] - running[None, :]
        mixing = jnp.where(lower_mask, jnp.exp(jnp.where(lower_mask, log_gaps, 0.0)), 0.0)
        affinity = jnp.einsum('ign,jgn->ijg', read_f, key_f, precision=HIGHEST)
        weights = to_bf16_and_back(affinity[..., None] * mixing * step_blk[None])
        output = jnp.einsum('ijgr,jgrp->igrp', weights, value_f, precision=HIGHEST)
        output = output + jnp.einsum('ign,grpn,igr->igrp', read_f, carried, jnp.exp(running), precision=HIGHEST)
        to_end = jnp.exp(running[-1:] - running) * step_blk
        state_in = to_bf16_and_back(key_f[:, :, None, :] * to_end[..., None])
        carried = jnp.exp(running[-1])[..., None, None] * carried + jnp.einsum('jgrn,jgrp->grpn', state_in, value_f, precision=HIGHEST)
        return (carried, output)
    final_state, outputs = lax.scan(advance, start_state, (values, steps_blk, decays, keys_b, reads_c))
    return (outputs.reshape(length, groups, repeat, HEAD_DIM), final_state)

def group_norm(combined, out_gain):
    length, groups, repeat, _ = combined.shape
    mean_square = lax.optimization_barrier(jnp.mean(combined * combined, axis=(2, 3), keepdims=True))
    scaled = combined * lax.rsqrt(mean_square + GROUP_EPS) * out_gain.astype(jnp.float32).reshape(groups, repeat, HEAD_DIM)
    return scaled.reshape(length, groups * repeat * HEAD_DIM).astype(jnp.bfloat16)

def reference(latent, cond, context, context_cond, modulation, norm_gain, w_x, w_gate, w_b, w_c, w_dt, conv_x, conv_b, conv_c, decay_rate, decay_extra, out_gain, w_out):
    model_width = latent.shape[1]
    cond_rows = jax.nn.silu(jnp.stack([cond, context_cond]).astype(jnp.float32)).astype(jnp.bfloat16)
    mod_rows = jnp.dot(cond_rows, modulation, preferred_element_type=jnp.float32)
    shift_rows = mod_rows[:, :model_width]
    scale_rows = mod_rows[:, model_width:2 * model_width]
    gate_row = mod_rows[0, 2 * model_width:]
    hidden = modulated_norm(latent, norm_gain, shift_rows[0], scale_rows[0])
    context_hidden = modulated_norm(context, norm_gain, shift_rows[1], scale_rows[1])
    ctx_xs = short_conv(project(context_hidden, w_x), conv_x)
    ctx_bmat = short_conv(project(context_hidden, w_b), conv_b)
    ctx_dt = jnp.stack([jax.nn.softplus(project(context_hidden, w_dt[direction]).astype(jnp.float32)) for direction in range(2)])
    forward_start, backward_start = context_states(ctx_xs, ctx_bmat, ctx_dt, decay_rate)
    latent_xs = short_conv(project(hidden, w_x), conv_x)
    latent_b = short_conv(project(hidden, w_b), conv_b)
    latent_c = short_conv(project(hidden, w_c), conv_c)
    gate_in = project(hidden, w_gate)
    latent_dt = jnp.stack([jax.nn.softplus(project(hidden, w_dt[direction]).astype(jnp.float32)) for direction in range(2)])
    log_decay = -decay_rate[:, None, :] * latent_dt + decay_extra[None]
    y_forward, _ = block_pass(latent_xs, latent_dt[0], log_decay[0], latent_b, latent_c, forward_start)
    y_backward, _ = block_pass(latent_xs[::-1], latent_dt[1][::-1], log_decay[1][::-1], latent_b[::-1], latent_c[::-1], backward_start)
    length, groups, repeat, _ = y_forward.shape
    gate_act = jax.nn.silu(gate_in.astype(jnp.float32)).reshape(length, groups, repeat, HEAD_DIM)
    combined = (y_forward + y_backward[::-1]) * gate_act
    normed = group_norm(combined, out_gain)
    branch = jnp.dot(normed, w_out, preferred_element_type=jnp.float32)
    return (latent.astype(jnp.float32) + gate_row * branch).astype(jnp.bfloat16)
```

```python
import jax
import jax.numpy as jnp
import numpy as np
from jax import lax
from jax.sharding import Mesh
from jax.sharding import PartitionSpec as P

HEAD_DIM = 64
STATE = 64
ROW_EPS = 1e-06
GROUP_EPS = 1e-05
HIGHEST = lax.Precision.HIGHEST
F32 = jnp.float32
BF16 = jnp.bfloat16
PAD = 8

SP = ("za", "zb", "zc")
NEAR = ("zb", "zc")
MOD_NEAR = ("zc", "tp")
MOD_FAR = ("za", "zb")


def exchange(x, axis):
    return lax.all_to_all(x, axis, 0, 0, tiled=True)


def share(x, axis):
    n = lax.axis_size(axis)
    full = jnp.broadcast_to(x[None], (n, *x.shape)).reshape(n * x.shape[0], *x.shape[1:])
    return exchange(full, axis).reshape(n, *x.shape)


def split_hi_lo(x):
    hi = lax.reduce_precision(x, 8, 7)
    return hi, x - hi


def mod_vectors(cond, context_cond, modulation):
    share_rows = modulation.shape[0]
    width = modulation.shape[1] // 3
    rows = jax.nn.silu(jnp.stack([cond, context_cond]).astype(F32)).astype(BF16)
    own = lax.dynamic_slice_in_dim(rows, lax.axis_index((*SP, "tp")) * share_rows, share_rows, 1)
    part = jnp.dot(own, modulation, preferred_element_type=F32)
    n = lax.axis_size(MOD_NEAR)
    cut = width // n
    pairs = 5 * cut // 256
    part = part.reshape(6, n, cut)[:5].transpose(1, 0, 2).reshape(n * pairs, 2, 128)
    part = jnp.sum(exchange(part, MOD_NEAR).reshape(n, pairs, 2, 128), axis=0)
    part = jnp.sum(share(part, MOD_FAR), axis=0)
    full = share(part, MOD_NEAR)
    return full.reshape(n, 5, cut).transpose(1, 0, 2).reshape(5, width)


def modulated_norm(rows, norm_gain, shift_row, scale_row):
    values = rows.astype(F32)
    normed = values * lax.rsqrt(jnp.mean(values * values, axis=-1, keepdims=True) + ROW_EPS)
    return (normed * norm_gain.astype(F32) * (1.0 + scale_row) + shift_row).astype(BF16)


def conv(values, taps, first, length):
    total = jnp.zeros((length, values.shape[1]), F32)
    for k in range(4):
        total = total + taps[k].astype(F32) * values[first + k : first + k + length]
    return jax.nn.silu(total).astype(BF16)


def wide(v):
    heads = v.shape[1] // 2
    v = v.reshape(v.shape[0], 2, heads).transpose(0, 2, 1)
    return jnp.repeat(v, HEAD_DIM, axis=2).reshape(v.shape[0], heads * 2 * HEAD_DIM)


def twice(x):
    heads = x.shape[1] // HEAD_DIM
    v = x.reshape(x.shape[0], heads, 1, HEAD_DIM)
    return jnp.broadcast_to(v, (x.shape[0], heads, 2, HEAD_DIM)).reshape(x.shape[0], heads * 2 * HEAD_DIM)


def running_sums(log_decay):
    length = log_decay.shape[0]
    heads = log_decay.shape[1] // 2
    i = jnp.arange(length)
    low = (i[:, None] >= i[None, :]).astype(F32)
    forward = jnp.dot(low, log_decay[:, :heads], precision=HIGHEST)
    backward = jnp.dot(low.T, log_decay[:, heads:], precision=HIGHEST)
    return jnp.concatenate([forward, backward], axis=1)


def end_states(xs, bmat, dt, running, total):
    weights = wide(jnp.exp(total - running) * dt)
    weighted = (twice(xs).astype(F32) * weights).astype(BF16)
    return lax.dot_general(bmat, weighted, (((0,), (0,)), ((), ())), preferred_element_type=F32)


def before_products(totals, f_lane):
    run = jnp.cumsum(totals, axis=0)
    return jnp.where(f_lane, run[-1:] - run, run - totals)


def entry_states(ctx_state, ctx_total, lat_state, lat_total):
    heads = ctx_total.shape[1] // 2
    n = lax.axis_size(NEAR)
    half = heads * STATE // n

    def pieces(state):
        v = state.reshape(STATE // half, half, heads, 128).transpose(2, 0, 1, 3)
        return v.reshape(n, half, 128)

    decays = []
    for total in (ctx_total, lat_total):
        w = jnp.repeat(wide(total).reshape(heads, 1, 128), STATE // half, axis=0)
        decays += list(split_hi_lo(w))
    decays.append(jnp.zeros((n, 4, 128), F32))
    near = jnp.concatenate([pieces(ctx_state), pieces(lat_state), *decays], axis=1).astype(BF16)
    near = exchange(near, NEAR).astype(F32)
    f_lane = lax.broadcasted_iota(jnp.int32, (1, 128), 1) < HEAD_DIM
    group, member_total = [], None
    for k in range(2):
        states = near[:, k * half : (k + 1) * half]
        totals = near[:, 2 * half + 2 * k] + near[:, 2 * half + 2 * k + 1]
        group.append(jnp.sum(jnp.exp(before_products(totals, f_lane))[:, None] * states, axis=0))
        member_total = totals
        group.append(jnp.sum(totals, axis=0, keepdims=True))
    member_state = near[:, half : 2 * half]
    far = jnp.concatenate(
        [group[0], group[2], *split_hi_lo(group[1]), *split_hi_lo(group[3]), jnp.zeros((4, 128), F32)], axis=0
    ).astype(BF16)
    far = share(far, "za").astype(F32)
    count = far.shape[0]
    ctx_g, lat_g = far[:, :half], far[:, half : 2 * half]
    ctx_t = far[:, 2 * half] + far[:, 2 * half + 1]
    lat_t = far[:, 2 * half + 2] + far[:, 2 * half + 3]
    entry = jnp.sum(jnp.exp(before_products(ctx_t, f_lane))[:, None] * ctx_g, axis=0)
    place = lax.axis_index("za")
    for s in range(count - 1):
        keep = jnp.where(f_lane, s < place, count - 1 - s > place)
        total = jnp.where(f_lane, lat_t[s], lat_t[count - 1 - s])
        state = jnp.where(f_lane, lat_g[s], lat_g[count - 1 - s])
        entry = jnp.where(keep, jnp.exp(total) * entry + state, entry)
    entries = [entry]
    for s in range(n - 1):
        total = jnp.where(f_lane, member_total[s], member_total[n - 1 - s])
        state = jnp.where(f_lane, member_state[s], member_state[n - 1 - s])
        entry = jnp.exp(total) * entry + state
        entries.append(entry)
    back = jnp.stack([jnp.where(f_lane, entries[m], entries[n - 1 - m]) for m in range(n)]).astype(BF16)
    back = exchange(back, NEAR)
    return back.reshape(heads, STATE, 128)


def local(
    latent,
    cond,
    context,
    context_cond,
    modulation,
    norm_gain,
    w_x,
    w_gate,
    w_b,
    w_c,
    w_dt,
    conv_x,
    conv_b,
    conv_c,
    decay_rate,
    decay_extra,
    out_gain,
    w_out,
):
    heads = w_dt.shape[2]
    head_cols = w_x.shape[1]
    tokens = decay_extra.shape[0]
    ctx_tokens = context.shape[0]
    mods = mod_vectors(cond, context_cond, modulation)

    block = share(latent, "tp").reshape(tokens, latent.shape[1])
    count = lax.axis_size(SP)
    place = lax.axis_index(SP)
    up = [(i, i + 1) for i in range(count - 1)]
    down = [(i + 1, i) for i in range(count - 1)]
    low = lax.ppermute(jnp.concatenate([block[-PAD:], context[-PAD:]]), SP, up)
    high = lax.ppermute(jnp.concatenate([block[:PAD], context[:PAD]]), SP, down)
    latent_rows = jnp.concatenate([low[:PAD], block, high[:PAD]])
    context_rows = jnp.concatenate([low[PAD:], context, high[PAD:]])

    lat_len = tokens + 2 * PAD
    hidden = jnp.concatenate(
        [
            modulated_norm(latent_rows, norm_gain, mods[0], mods[1]),
            modulated_norm(context_rows, norm_gain, mods[3], mods[4]),
        ]
    )
    row = jnp.arange(hidden.shape[0])
    first = (row < PAD) | ((row >= lat_len) & (row < lat_len + PAD))
    last = ((row >= lat_len - PAD) & (row < lat_len)) | (row >= hidden.shape[0] - PAD)
    outside = (first & (place == 0)) | (last & (place == count - 1))
    inner = hidden[PAD : PAD + tokens]

    def project(rows, weight):
        return jnp.dot(rows, weight, preferred_element_type=F32).astype(BF16)

    p_x = jnp.where(outside[:, None], 0.0, project(hidden, w_x).astype(F32))
    p_b = jnp.where(outside[:, None], 0.0, project(hidden, w_b).astype(F32))
    p_c = jnp.where(outside[:lat_len, None], 0.0, project(hidden[:lat_len], w_c).astype(F32))
    p_dt = jax.nn.softplus(project(hidden, jnp.concatenate([w_dt[0], w_dt[1]], axis=1)).astype(F32))
    z = project(inner, w_gate).astype(F32)

    off = PAD - 2
    xs = conv(p_x, conv_x, off, tokens)
    bmat = conv(p_b, conv_b, off, tokens)
    cmat = conv(p_c, conv_c, off, tokens)
    ctx_xs = conv(p_x, conv_x, lat_len + off, ctx_tokens)
    ctx_b = conv(p_b, conv_b, lat_len + off, ctx_tokens)
    dt = p_dt[PAD : PAD + tokens]
    ctx_dt = p_dt[lat_len + PAD : lat_len + PAD + ctx_tokens]
    rate = decay_rate.reshape(1, 2 * heads)
    log_decay = -rate * dt + jnp.concatenate([decay_extra, decay_extra], axis=1)
    ctx_log_decay = -rate * ctx_dt
    running = running_sums(log_decay)
    ctx_running = running_sums(ctx_log_decay)
    total = jnp.sum(log_decay, axis=0, keepdims=True)
    ctx_total = jnp.sum(ctx_log_decay, axis=0, keepdims=True)
    entry = entry_states(
        end_states(ctx_xs, ctx_b, ctx_dt, ctx_running, ctx_total),
        ctx_total,
        end_states(xs, bmat, dt, running, total),
        total,
    )

    affinity = lax.dot_general(cmat, bmat, (((1,), (1,)), ((), ())), preferred_element_type=F32)
    i = jnp.arange(tokens)
    lower = i[:, None] >= i[None, :]
    upper = i[:, None] <= i[None, :]
    parts = []
    for h in range(heads):
        weights = jnp.zeros((tokens, tokens), F32)
        for d, mask in ((0, lower), (1, upper)):
            col = d * heads + h
            gap = running[:, col][:, None] - running[:, col][None, :]
            mixing = jnp.where(mask, jnp.exp(jnp.where(mask, gap, 0.0)), 0.0)
            weights = weights + mixing * dt[:, col][None, :]
        weights = (affinity * weights).astype(BF16)
        parts.append(jnp.dot(weights, xs[:, h * HEAD_DIM : (h + 1) * HEAD_DIM], preferred_element_type=F32))
    y = jnp.concatenate(parts, axis=1)
    flat = entry.transpose(1, 0, 2).reshape(STATE, heads * 128)
    carried = jnp.dot(cmat, flat, preferred_element_type=F32) * wide(jnp.exp(running))
    carried = carried.reshape(tokens, heads, 2, HEAD_DIM)
    y = y + (carried[:, :, 0] + carried[:, :, 1]).reshape(tokens, heads * HEAD_DIM)
    gated = y * jax.nn.silu(z)
    mean_square = jnp.mean(gated * gated, axis=1, keepdims=True)
    normed = (gated * lax.rsqrt(mean_square + GROUP_EPS) * out_gain.astype(F32)).astype(BF16)
    tp_count = lax.axis_size("tp")
    stacked = normed.reshape(tp_count, tokens // tp_count, head_cols)
    full = lax.all_to_all(stacked, "tp", split_axis=0, concat_axis=2, tiled=True)[0]
    branch = jnp.dot(full, w_out, preferred_element_type=F32)
    return (latent.astype(F32) + mods[2] * branch).astype(BF16)


def solution(mesh):
    sp, tp, dp = (mesh.shape[a] for a in ("sp", "tp", "dp"))
    inner = Mesh(np.asarray(mesh.devices).reshape(sp // 8, 4, 2, tp, dp), (*SP, "tp", "dp"))
    in_specs = (
        P(("dp", *SP, "tp"), None),
        P("dp"),
        P(("dp", *SP), None),
        P(),
        P((*SP, "tp"), None),
        P(),
        P(None, "tp"),
        P(None, "tp"),
        P(None, "tp"),
        P(None, "tp"),
        P(None, None, "tp"),
        P(None, "tp"),
        P(None, "tp"),
        P(None, "tp"),
        P(None, "tp"),
        P(("dp", *SP), "tp"),
        P("tp"),
        P(),
    )
    out_specs = P(("dp", *SP, "tp"), None)
    return jax.shard_map(local, mesh=inner, in_specs=in_specs, out_specs=out_specs, check_vma=False)
```

```python
import jax
import jax.numpy as jnp
import numpy as np
from jax import lax
from jax.sharding import Mesh
from jax.sharding import PartitionSpec as P


HEAD_DIM = 64
STATE = 64
ROW_EPS = 1e-06
GROUP_EPS = 1e-05
HIGHEST = lax.Precision.HIGHEST
F32 = jnp.float32
BF16 = jnp.bfloat16
PAD = 8

SP = ("za", "zb", "zc")
NEAR = ("zb", "zc")
MOD_NEAR = ("zc", "tp")
MOD_FAR = ("za", "zb")


def exchange(x, axis):
    return lax.all_to_all(x, axis, 0, 0, tiled=True)


def share(x, axis):
    n = lax.axis_size(axis)
    full = jnp.broadcast_to(x[None], (n, *x.shape)).reshape(n * x.shape[0], *x.shape[1:])
    return exchange(full, axis).reshape(n, *x.shape)


def ring_rows(x):
    n = lax.axis_size("tp")
    moved = [x] + [lax.ppermute(x, "tp", [(i, (i + k) % n) for i in range(n)]) for k in range(1, n)]
    moved = jnp.stack(moved)
    place = lax.axis_index("tp")
    return jnp.stack([lax.dynamic_index_in_dim(moved, (place - t) % n, 0, False) for t in range(n)])


def split_hi_lo(x):
    hi = lax.reduce_precision(x, 8, 7)
    return hi, x - hi


def mod_vectors(cond, context_cond, modulation, own_rows):
    share_rows = modulation.shape[0]
    width = modulation.shape[1] // 3
    rows = jax.nn.silu(jnp.stack([cond, context_cond]).astype(F32)).astype(BF16)
    own = lax.dynamic_slice_in_dim(rows, lax.axis_index((*SP, "tp")) * share_rows, share_rows, 1)
    part = jnp.dot(own, modulation, preferred_element_type=F32)
    n = lax.axis_size(MOD_NEAR)
    cut = width // n
    pairs = 5 * cut // 256
    part = part.reshape(6, n, cut)[:5].transpose(1, 0, 2).reshape(n * pairs, 2, 128)
    part = jnp.sum(exchange(part, MOD_NEAR).reshape(n, pairs, 2, 128), axis=0)
    part, own_rows = lax.optimization_barrier((part, own_rows))
    far = share(part, MOD_FAR)
    gathered = ring_rows(own_rows)
    full = share(jnp.sum(far, axis=0), MOD_NEAR)
    return full.reshape(n, 5, cut).transpose(1, 0, 2).reshape(5, width), gathered


def modulated_norm(rows, norm_gain, shift_row, scale_row):
    values = rows.astype(F32)
    normed = values * lax.rsqrt(jnp.mean(values * values, axis=-1, keepdims=True) + ROW_EPS)
    return (normed * norm_gain.astype(F32) * (1.0 + scale_row) + shift_row).astype(BF16)


def conv(values, taps, first, length):
    total = jnp.zeros((length, values.shape[1]), F32)
    for k in range(4):
        total = total + taps[k].astype(F32) * values[first + k : first + k + length]
    return jax.nn.silu(total).astype(BF16)


def wide(v):
    heads = v.shape[1] // 2
    v = v.reshape(v.shape[0], 2, heads).transpose(0, 2, 1)
    return jnp.repeat(v, HEAD_DIM, axis=2).reshape(v.shape[0], heads * 2 * HEAD_DIM)


def twice(x):
    heads = x.shape[1] // HEAD_DIM
    v = x.reshape(x.shape[0], heads, 1, HEAD_DIM)
    return jnp.broadcast_to(v, (x.shape[0], heads, 2, HEAD_DIM)).reshape(x.shape[0], heads * 2 * HEAD_DIM)


def running_sums(log_decay):
    length = log_decay.shape[0]
    heads = log_decay.shape[1] // 2
    i = jnp.arange(length)
    low = (i[:, None] >= i[None, :]).astype(F32)
    forward = jnp.dot(low, log_decay[:, :heads], precision=HIGHEST)
    backward = jnp.dot(low.T, log_decay[:, heads:], precision=HIGHEST)
    return jnp.concatenate([forward, backward], axis=1)


def end_states(xs, bmat, dt, running, total):
    weights = wide(jnp.exp(total - running) * dt)
    weighted = (twice(xs).astype(F32) * weights).astype(BF16)
    return lax.dot_general(bmat, weighted, (((0,), (0,)), ((), ())), preferred_element_type=F32)


def entry_sums(states, totals, f_lane):
    n = states.shape[0]
    m = lax.broadcasted_iota(jnp.int32, (n + 1, n, n, 1), 0)
    k = lax.broadcasted_iota(jnp.int32, (n + 1, n, n, 1), 1)
    j = lax.broadcasted_iota(jnp.int32, (n + 1, n, n, 1), 2)
    mb = jnp.where(m == n, -1, m)
    between = jnp.where(f_lane, (j > k) & (j < m), (j < k) & (j > mb))
    gap = jnp.sum(jnp.where(between, totals[None, None], 0.0), axis=2)
    ahead = jnp.where(f_lane, k[:, :, 0] < m[:, :, 0], k[:, :, 0] > mb[:, :, 0])
    factor = jnp.where(ahead, jnp.exp(gap), 0.0)
    sums = jnp.sum(factor[:, :, None] * states[None], axis=1)
    to_m = jnp.sum(jnp.where(ahead, totals[None], 0.0), axis=1)
    return sums, to_m


def entry_states(ctx_state, ctx_total, lat_state, lat_total):
    heads = ctx_total.shape[1] // 2
    n = lax.axis_size(NEAR)
    half = heads * STATE // n

    def pieces(state):
        v = state.reshape(STATE // half, half, heads, 128).transpose(2, 0, 1, 3)
        return v.reshape(n, half, 128)

    decays = []
    for total in (ctx_total, lat_total):
        w = jnp.repeat(wide(total).reshape(heads, 1, 128), STATE // half, axis=0)
        decays += list(split_hi_lo(w))
    decays.append(jnp.zeros((n, 4, 128), F32))
    near = jnp.concatenate([pieces(ctx_state), pieces(lat_state), *decays], axis=1).astype(BF16)
    near = exchange(near, NEAR).astype(F32)
    f_lane = lax.broadcasted_iota(jnp.int32, (1, 128), 1) < HEAD_DIM
    ctx_t = near[:, 2 * half] + near[:, 2 * half + 1]
    lat_t = near[:, 2 * half + 2] + near[:, 2 * half + 3]
    ctx_sums, ctx_to = entry_sums(near[:, :half], ctx_t, f_lane)
    lat_sums, lat_to = entry_sums(near[:, half : 2 * half], lat_t, f_lane)
    far = jnp.concatenate(
        [ctx_sums[n], lat_sums[n], *split_hi_lo(ctx_to[n:]), *split_hi_lo(lat_to[n:]), jnp.zeros((4, 128), F32)], axis=0
    ).astype(BF16)
    far = share(far, "za").astype(F32)
    count = far.shape[0]
    start, _ = entry_sums(far[:, :half], far[:, 2 * half] + far[:, 2 * half + 1], f_lane)
    group, group_to = entry_sums(far[:, half : 2 * half], far[:, 2 * half + 2] + far[:, 2 * half + 3], f_lane)
    mine = (jnp.arange(count + 1) == lax.axis_index("za")).astype(F32)
    group = jnp.sum(mine[:, None, None] * group, axis=0)
    group_to = jnp.sum(mine[:, None] * group_to, axis=0)
    entry = jnp.exp(group_to) * start[count] + group
    back = (jnp.exp(lat_to[:n, None]) * entry + lat_sums[:n]).astype(BF16)
    back = exchange(back, NEAR)
    return back.reshape(heads, STATE, 128)


def program(
    latent,
    cond,
    context,
    context_cond,
    modulation,
    norm_gain,
    w_x,
    w_gate,
    w_b,
    w_c,
    w_dt,
    conv_x,
    conv_b,
    conv_c,
    decay_rate,
    decay_extra,
    out_gain,
    w_out,
):
    heads = w_dt.shape[2]
    head_cols = w_x.shape[1]
    tokens = decay_extra.shape[0]
    ctx_tokens = context.shape[0]
    count = lax.axis_size(SP)
    place = lax.axis_index(SP)
    up = [(i, i + 1) for i in range(count - 1)]
    down = [(i + 1, i) for i in range(count - 1)]
    low = lax.ppermute(jnp.concatenate([latent[-PAD:], context[-PAD:]]), SP, up)
    high = lax.ppermute(jnp.concatenate([latent[:PAD], context[:PAD]]), SP, down)
    own = jnp.concatenate([latent, low[:PAD], high[:PAD]])
    mods, gathered = mod_vectors(cond, context_cond, modulation, own)
    tokens_own = latent.shape[0]
    latent_rows = jnp.concatenate(
        [
            gathered[-1, tokens_own : tokens_own + PAD],
            gathered[:, :tokens_own].reshape(tokens, latent.shape[1]),
            gathered[0, tokens_own + PAD :],
        ]
    )
    context_rows = jnp.concatenate([low[PAD:], context, high[PAD:]])

    lat_len = tokens + 2 * PAD
    hidden = jnp.concatenate(
        [
            modulated_norm(latent_rows, norm_gain, mods[0], mods[1]),
            modulated_norm(context_rows, norm_gain, mods[3], mods[4]),
        ]
    )
    row = jnp.arange(hidden.shape[0])
    first = (row < PAD) | ((row >= lat_len) & (row < lat_len + PAD))
    last = ((row >= lat_len - PAD) & (row < lat_len)) | (row >= hidden.shape[0] - PAD)
    outside = (first & (place == 0)) | (last & (place == count - 1))
    inner = hidden[PAD : PAD + tokens]

    def project(rows, weight):
        return jnp.dot(rows, weight, preferred_element_type=F32).astype(BF16)

    p_x = jnp.where(outside[:, None], 0.0, project(hidden, w_x).astype(F32))
    p_b = jnp.where(outside[:, None], 0.0, project(hidden, w_b).astype(F32))
    p_c = jnp.where(outside[:lat_len, None], 0.0, project(hidden[:lat_len], w_c).astype(F32))
    p_dt = jax.nn.softplus(project(hidden, jnp.concatenate([w_dt[0], w_dt[1]], axis=1)).astype(F32))
    z = project(inner, w_gate).astype(F32)

    off = PAD - 2
    xs = conv(p_x, conv_x, off, tokens)
    bmat = conv(p_b, conv_b, off, tokens)
    cmat = conv(p_c, conv_c, off, tokens)
    ctx_xs = conv(p_x, conv_x, lat_len + off, ctx_tokens)
    ctx_b = conv(p_b, conv_b, lat_len + off, ctx_tokens)
    dt = p_dt[PAD : PAD + tokens]
    ctx_dt = p_dt[lat_len + PAD : lat_len + PAD + ctx_tokens]
    rate = decay_rate.reshape(1, 2 * heads)
    log_decay = -rate * dt + jnp.concatenate([decay_extra, decay_extra], axis=1)
    ctx_log_decay = -rate * ctx_dt
    running = running_sums(log_decay)
    ctx_running = running_sums(ctx_log_decay)
    total = jnp.sum(log_decay, axis=0, keepdims=True)
    ctx_total = jnp.sum(ctx_log_decay, axis=0, keepdims=True)
    entry = entry_states(
        end_states(ctx_xs, ctx_b, ctx_dt, ctx_running, ctx_total),
        ctx_total,
        end_states(xs, bmat, dt, running, total),
        total,
    )

    affinity = lax.dot_general(cmat, bmat, (((1,), (1,)), ((), ())), preferred_element_type=F32)
    i = jnp.arange(tokens)
    lower = i[:, None] >= i[None, :]
    upper = i[:, None] <= i[None, :]
    parts = []
    for h in range(heads):
        weights = jnp.zeros((tokens, tokens), F32)
        for d, mask in ((0, lower), (1, upper)):
            col = d * heads + h
            gap = running[:, col][:, None] - running[:, col][None, :]
            mixing = jnp.where(mask, jnp.exp(jnp.where(mask, gap, 0.0)), 0.0)
            weights = weights + mixing * dt[:, col][None, :]
        weights = (affinity * weights).astype(BF16)
        parts.append(jnp.dot(weights, xs[:, h * HEAD_DIM : (h + 1) * HEAD_DIM], preferred_element_type=F32))
    y = jnp.concatenate(parts, axis=1)
    flat = entry.transpose(1, 0, 2).reshape(STATE, heads * 128)
    carried = jnp.dot(cmat, flat, preferred_element_type=F32) * wide(jnp.exp(running))
    carried = carried.reshape(tokens, heads, 2, HEAD_DIM)
    y = y + (carried[:, :, 0] + carried[:, :, 1]).reshape(tokens, heads * HEAD_DIM)
    gated = y * jax.nn.silu(z)
    mean_square = jnp.mean(gated * gated, axis=1, keepdims=True)
    normed = (gated * lax.rsqrt(mean_square + GROUP_EPS) * out_gain.astype(F32)).astype(BF16)
    tp_count = lax.axis_size("tp")
    stacked = normed.reshape(tp_count, tokens // tp_count, head_cols)
    full = lax.all_to_all(stacked, "tp", split_axis=0, concat_axis=2, tiled=True)[0]
    branch = jnp.dot(full, w_out, preferred_element_type=F32)
    return (latent.astype(F32) + mods[2] * branch).astype(BF16)


def solution(mesh):
    sp, tp, dp = (mesh.shape[a] for a in ("sp", "tp", "dp"))
    inner = Mesh(np.asarray(mesh.devices).reshape(sp // 8, 4, 2, tp, dp), (*SP, "tp", "dp"))
    in_specs = (
        P(("dp", *SP, "tp"), None),
        P("dp"),
        P(("dp", *SP), None),
        P(),
        P((*SP, "tp"), None),
        P(),
        P(None, "tp"),
        P(None, "tp"),
        P(None, "tp"),
        P(None, "tp"),
        P(None, None, "tp"),
        P(None, "tp"),
        P(None, "tp"),
        P(None, "tp"),
        P(None, "tp"),
        P(("dp", *SP), "tp"),
        P("tp"),
        P(),
    )
    out_specs = P(("dp", *SP, "tp"), None)
    return jax.shard_map(program, mesh=inner, in_specs=in_specs, out_specs=out_specs, check_vma=False)
```

```python
import jax
import jax.numpy as jnp
import numpy as np
from jax import lax
from jax.experimental import pallas as pl
from jax.experimental.pallas import tpu as pltpu
from jax.sharding import Mesh
from jax.sharding import PartitionSpec as P


HEAD_DIM = 64
STATE = 64
ROW_EPS = 1e-06
GROUP_EPS = 1e-05
HIGHEST = lax.Precision.HIGHEST
F32 = jnp.float32
BF16 = jnp.bfloat16
PAD = 8

SP = ("za", "zb", "zc")
NEAR = ("zb", "zc")
MOD_NEAR = ("zc", "tp")
MOD_FAR = ("za", "zb")


def exchange(x, axis):
    return lax.all_to_all(x, axis, 0, 0, tiled=True)


def share(x, axis):
    n = lax.axis_size(axis)
    full = jnp.broadcast_to(x[None], (n, *x.shape)).reshape(n * x.shape[0], *x.shape[1:])
    return exchange(full, axis).reshape(n, *x.shape)


def ring_rows(x):
    n = lax.axis_size("tp")
    moved = [x] + [lax.ppermute(x, "tp", [(i, (i + k) % n) for i in range(n)]) for k in range(1, n)]
    moved = jnp.stack(moved)
    place = lax.axis_index("tp")
    return jnp.stack([lax.dynamic_index_in_dim(moved, (place - t) % n, 0, False) for t in range(n)])


def split_hi_lo(x):
    hi = lax.reduce_precision(x, 8, 7)
    return hi, x - hi


def silu(v):
    return v / (1.0 + jnp.exp(-v))


def partial_kernel(first, cond, context_cond, modulation, out):
    share_rows, cols = modulation.shape
    width = cols // 3
    at = first[0] + lax.broadcasted_iota(jnp.int32, (share_rows, width), 0)
    pick = jnp.where(lax.broadcasted_iota(jnp.int32, (share_rows, width), 1) == at, 1.0, 0.0).astype(BF16)
    table = modulation[...]
    cut = width // (out.shape[0] // 5)
    for source, kinds in ((0, (0, 1, 2)), (1, (0, 1))):
        v = (cond, context_cond)[source][...].astype(F32)
        row = silu(v).astype(BF16)
        own = lax.dot_general(row, pick, (((1,), (1,)), ((), ())), preferred_element_type=F32).astype(BF16)
        sums = jnp.dot(own, table, preferred_element_type=F32)
        for kind in kinds:
            for n in range(width // cut):
                for r in range(2):
                    at = kind * width + n * cut + r * 128
                    out[n * 5 + 3 * source + kind, r : r + 1, :] = sums[0:1, at : at + 128]


def partial_mods(first, cond, context_cond, modulation, n):
    vmem = pl.BlockSpec(memory_space=pltpu.VMEM)
    width = modulation.shape[1] // 3
    return pl.pallas_call(
        partial_kernel,
        out_shape=jax.ShapeDtypeStruct((n * 5, 2, 128), F32),
        in_specs=[pl.BlockSpec(memory_space=pltpu.SMEM), vmem, vmem, vmem],
        out_specs=vmem,
        compiler_params=pltpu.CompilerParams(vmem_limit_bytes=8 * 2**20),
        name="partial_mods",
    )(
        first.astype(jnp.int32).reshape(1),
        jnp.broadcast_to(cond[None], (8, width)),
        jnp.broadcast_to(context_cond[None], (8, width)),
        modulation,
    )


def mod_vectors(cond, context_cond, modulation, own_rows):
    share_rows = modulation.shape[0]
    width = modulation.shape[1] // 3
    n = lax.axis_size(MOD_NEAR)
    pairs = 5 * (width // n) // 256
    first = lax.axis_index((*SP, "tp")) * share_rows
    part = partial_mods(first, cond, context_cond, modulation, n)
    part = jnp.sum(exchange(part, MOD_NEAR).reshape(n, pairs, 2, 128), axis=0)
    part, own_rows = lax.optimization_barrier((part, own_rows))
    far = share(part, MOD_FAR)
    gathered = ring_rows(own_rows)
    full = share(jnp.sum(far, axis=0), MOD_NEAR)
    return full.reshape(n * pairs, 2, 128), gathered


def wide(v):
    heads = v.shape[1] // 2
    v = v.reshape(v.shape[0], 2, heads).transpose(0, 2, 1)
    return jnp.repeat(v, HEAD_DIM, axis=2).reshape(v.shape[0], heads * 2 * HEAD_DIM)


def front_kernel(
    edge, rows, mods, gain, w_dt, taps, rate, extra, w_x, w_g, w_bc,
    near, xs_out, bc_out, z_out, run_out, dt_out, gate_out,
    hid, buf_x, buf_g, buf_bc, proj, sems,
):
    copies = [
        pltpu.make_async_copy(src, dst, sems.at[i])
        for i, (src, dst) in enumerate(((w_x, buf_x), (w_bc, buf_bc), (w_g, buf_g)))
    ]
    for c in copies:
        c.start()
    total_rows, _ = rows.shape
    tokens = xs_out.shape[0]
    lat_rows = tokens + 2 * PAD
    ctx = total_rows - lat_rows - 2 * PAD
    chunks = mods.shape[0] // 5

    def vector(kind):
        return jnp.concatenate([mods[n * 5 + kind, r : r + 1, :] for n in range(chunks) for r in range(2)], axis=1)

    gate_out[...] = vector(2)
    g = gain[...].astype(F32)
    for first, count, shift, scale in ((0, lat_rows, 0, 1), (lat_rows, total_rows - lat_rows, 3, 4)):
        shift_row = vector(shift)
        factor = g * (1.0 + vector(scale))

        def norm(i, _, first=first, shift_row=shift_row, factor=factor):
            at = pl.ds(pl.multiple_of(first + i * 16, 16), 16)
            v = rows[at, :].astype(F32)
            r = lax.rsqrt(jnp.mean(v * v, axis=1, keepdims=True) + ROW_EPS)
            hid[at, :] = (v * r * factor + shift_row).astype(BF16)
            return 0

        lax.fori_loop(0, count // 16, norm, 0)

    def rounded(v):
        return v.astype(BF16).astype(F32)

    hidden = hid[...]
    p_dt = lax.dot_general(hidden, w_dt[...], (((1,), (1,)), ((), ())), preferred_element_type=F32)
    copies[0].wait()
    p_x = rounded(jnp.dot(hidden, buf_x[...], preferred_element_type=F32))
    copies[1].wait()
    p_bc = rounded(jnp.dot(hidden, buf_bc[...], preferred_element_type=F32))
    row = lax.broadcasted_iota(jnp.int32, (total_rows, 1), 0)
    is_first = (row < PAD) | ((row >= lat_rows) & (row < lat_rows + PAD))
    is_last = ((row >= lat_rows - PAD) & (row < lat_rows)) | (row >= total_rows - PAD)
    outside = (is_first & (edge[0] == 1)) | (is_last & (edge[1] == 1))
    cols = p_x.shape[1]
    proj[:, :cols] = jnp.where(outside, 0.0, p_x)
    proj[:, cols:] = jnp.where(outside, 0.0, p_bc)

    def conv(first, length):
        acc = jnp.zeros((length, proj.shape[1]), F32)
        for k in range(4):
            acc = acc + taps[k : k + 1, :].astype(F32) * proj[first + k : first + k + length, :]
        return silu(acc).astype(BF16)

    lat_u = conv(PAD - 2, tokens)
    ctx_u = conv(lat_rows + PAD - 2, ctx)
    xs_out[...] = lat_u[:, :cols]
    bc_out[...] = lat_u[:, cols:]
    v = rounded(p_dt)
    p_dt = jnp.maximum(v, 0.0) + jnp.log1p(jnp.exp(-jnp.abs(v)))
    heads = extra.shape[1] // 2
    lane = lax.broadcasted_iota(jnp.int32, (1, 128), 1) < HEAD_DIM
    slots = near.shape[0]
    half = heads * STATE // slots
    rows8 = lax.broadcasted_iota(jnp.int32, (8, 1), 0)
    decays = []
    for u, dt, more, base in (
        (ctx_u, p_dt[lat_rows + PAD : lat_rows + PAD + ctx], None, 0),
        (lat_u, p_dt[PAD : PAD + tokens], extra, half),
    ):
        length = dt.shape[0]
        log_decay = -rate[...] * dt
        if more is not None:
            log_decay = log_decay + more[...]
        i = lax.broadcasted_iota(jnp.int32, (length, length), 0)
        j = lax.broadcasted_iota(jnp.int32, (length, length), 1)
        low = jnp.where(i >= j, 1.0, 0.0)
        high = jnp.where(i <= j, 1.0, 0.0)
        ahead = lax.broadcasted_iota(jnp.int32, (1, 2 * heads), 1) < heads
        running = jnp.where(
            ahead,
            jnp.dot(low, log_decay, precision=HIGHEST, preferred_element_type=F32),
            jnp.dot(high, log_decay, precision=HIGHEST, preferred_element_type=F32),
        )
        total = jnp.sum(log_decay, axis=0, keepdims=True)
        weight = jnp.exp(total - running) * dt
        if more is not None:
            run_out[...] = running
            dt_out[...] = dt
        bmat = u[:, cols : cols + STATE]
        here = []
        for h in range(heads):
            pair = u[:, 128 * (h // 2) : 128 * (h // 2) + 128].astype(F32)
            other = pltpu.roll(pair, HEAD_DIM, 1)
            twice = jnp.where(lane, pair, other) if h % 2 == 0 else jnp.where(lane, other, pair)
            w = jnp.where(lane, weight[:, h : h + 1], weight[:, heads + h : heads + h + 1])
            state = lax.dot_general(
                bmat, (twice * w).astype(BF16), (((0,), (0,)), ((), ())), preferred_element_type=F32
            ).astype(BF16)
            for part in range(STATE // half):
                near[h * (STATE // half) + part, base : base + half, :] = state[part * half : (part + 1) * half]
            here.append(jnp.where(lane, total[:, h : h + 1], total[:, heads + h : heads + h + 1]))
        decays.append(here)
    for h in range(heads):
        block = jnp.zeros((8, 128), F32)
        for k in range(2):
            t = decays[k][h]
            hi = rounded(t)
            block = jnp.where(rows8 == 2 * k, hi, jnp.where(rows8 == 2 * k + 1, t - hi, block))
        block = block.astype(BF16)
        for part in range(STATE // half):
            near[h * (STATE // half) + part, 2 * half :, :] = block
    copies[2].wait()
    z = rounded(jnp.dot(hid[PAD : PAD + tokens, :], buf_g[...], preferred_element_type=F32))
    z_out[...] = silu(z)


def front(edge, rows, mods, gain, w_dt, taps, rate, extra, w_x, w_g, w_bc, slots):
    tokens, heads2 = extra.shape
    cols = w_x.shape[1]
    width = rows.shape[1]
    vmem = pl.BlockSpec(memory_space=pltpu.VMEM)
    away = pl.BlockSpec(memory_space=pl.ANY)
    half = heads2 // 2 * STATE // slots
    shape = jax.ShapeDtypeStruct
    return pl.pallas_call(
        front_kernel,
        out_shape=(
            shape((slots, 2 * half + 8, 128), BF16),
            shape((tokens, cols), BF16),
            shape((tokens, w_bc.shape[1]), BF16),
            shape((tokens, cols), F32),
            shape((tokens, heads2), F32),
            shape((tokens, heads2), F32),
            shape((1, width), F32),
        ),
        in_specs=[pl.BlockSpec(memory_space=pltpu.SMEM)] + [vmem] * 7 + [away] * 3,
        out_specs=(vmem,) * 7,
        scratch_shapes=[
            pltpu.VMEM(rows.shape, BF16),
            pltpu.VMEM(w_x.shape, BF16),
            pltpu.VMEM(w_g.shape, BF16),
            pltpu.VMEM(w_bc.shape, BF16),
            pltpu.VMEM((rows.shape[0], cols + w_bc.shape[1]), F32),
            pltpu.SemaphoreType.DMA((3,)),
        ],
        compiler_params=pltpu.CompilerParams(vmem_limit_bytes=24 * 2**20),
        name="front",
    )(edge, rows, mods, gain, w_dt, taps, rate, extra, w_x, w_g, w_bc)


def last_kernel(parts, latent, gate, w_out, out, buf, sems):
    n, _, cols = parts.shape
    copies = [
        pltpu.make_async_copy(w_out.at[pl.ds(i * cols, cols)], buf.at[pl.ds(i * cols, cols)], sems.at[i])
        for i in range(n)
    ]
    for c in copies:
        c.start()
    acc = jnp.zeros(out.shape, F32)
    for i in range(n):
        copies[i].wait()
        acc = acc + jnp.dot(parts[i], buf[i * cols : (i + 1) * cols, :], preferred_element_type=F32)
    out[...] = (latent[...].astype(F32) + gate[...] * acc).astype(BF16)


def last(parts, latent, gate, w_out):
    vmem = pl.BlockSpec(memory_space=pltpu.VMEM)
    return pl.pallas_call(
        last_kernel,
        out_shape=jax.ShapeDtypeStruct(latent.shape, BF16),
        in_specs=[vmem, vmem, vmem, pl.BlockSpec(memory_space=pl.ANY)],
        out_specs=vmem,
        scratch_shapes=[pltpu.VMEM(w_out.shape, BF16), pltpu.SemaphoreType.DMA((parts.shape[0],))],
        compiler_params=pltpu.CompilerParams(vmem_limit_bytes=24 * 2**20),
        name="last",
    )(parts, latent, gate, w_out)


def entry_sums(states, totals, f_lane):
    n = states.shape[0]
    m = lax.broadcasted_iota(jnp.int32, (n + 1, n, n, 1), 0)
    k = lax.broadcasted_iota(jnp.int32, (n + 1, n, n, 1), 1)
    j = lax.broadcasted_iota(jnp.int32, (n + 1, n, n, 1), 2)
    mb = jnp.where(m == n, -1, m)
    between = jnp.where(f_lane, (j > k) & (j < m), (j < k) & (j > mb))
    gap = jnp.sum(jnp.where(between, totals[None, None], 0.0), axis=2)
    ahead = jnp.where(f_lane, k[:, :, 0] < m[:, :, 0], k[:, :, 0] > mb[:, :, 0])
    factor = jnp.where(ahead, jnp.exp(gap), 0.0)
    sums = jnp.sum(factor[:, :, None] * states[None], axis=1)
    to_m = jnp.sum(jnp.where(ahead, totals[None], 0.0), axis=1)
    return sums, to_m


def entry_states(near, heads):
    n = near.shape[0]
    half = heads * STATE // n
    near = exchange(near, NEAR).astype(F32)
    f_lane = lax.broadcasted_iota(jnp.int32, (1, 128), 1) < HEAD_DIM
    ctx_t = near[:, 2 * half] + near[:, 2 * half + 1]
    lat_t = near[:, 2 * half + 2] + near[:, 2 * half + 3]
    ctx_sums, ctx_to = entry_sums(near[:, :half], ctx_t, f_lane)
    lat_sums, lat_to = entry_sums(near[:, half : 2 * half], lat_t, f_lane)
    far = jnp.concatenate(
        [ctx_sums[n], lat_sums[n], *split_hi_lo(ctx_to[n:]), *split_hi_lo(lat_to[n:]), jnp.zeros((4, 128), F32)], axis=0
    ).astype(BF16)
    far = share(far, "za").astype(F32)
    count = far.shape[0]
    start, _ = entry_sums(far[:, :half], far[:, 2 * half] + far[:, 2 * half + 1], f_lane)
    group, group_to = entry_sums(far[:, half : 2 * half], far[:, 2 * half + 2] + far[:, 2 * half + 3], f_lane)
    mine = (jnp.arange(count + 1) == lax.axis_index("za")).astype(F32)
    group = jnp.sum(mine[:, None, None] * group, axis=0)
    group_to = jnp.sum(mine[:, None] * group_to, axis=0)
    entry = jnp.exp(group_to) * start[count] + group
    back = (jnp.exp(lat_to[:n, None]) * entry + lat_sums[:n]).astype(BF16)
    back = exchange(back, NEAR)
    return back.reshape(heads, STATE, 128)


def program(
    latent,
    cond,
    context,
    context_cond,
    modulation,
    norm_gain,
    w_x,
    w_gate,
    w_b,
    w_c,
    w_dt,
    conv_x,
    conv_b,
    conv_c,
    decay_rate,
    decay_extra,
    out_gain,
    w_out,
):
    heads = w_dt.shape[2]
    head_cols = w_x.shape[1]
    tokens = decay_extra.shape[0]
    count = lax.axis_size(SP)
    place = lax.axis_index(SP)
    up = [(i, i + 1) for i in range(count - 1)]
    down = [(i + 1, i) for i in range(count - 1)]
    low = lax.ppermute(jnp.concatenate([latent[-2:], context[-2:]]), SP, up)
    high = lax.ppermute(jnp.concatenate([latent[:1], context[:1]]), SP, down)

    def blank(n):
        return jnp.zeros((n, latent.shape[1]), BF16)

    own = jnp.concatenate([latent, low[:2], high[:1], blank(5)])
    mods, gathered = mod_vectors(cond, context_cond, modulation, own)
    tokens_own = latent.shape[0]
    rows = jnp.concatenate(
        [
            blank(PAD - 2),
            gathered[-1, tokens_own : tokens_own + 2],
            gathered[:, :tokens_own].reshape(tokens, latent.shape[1]),
            gathered[0, tokens_own + 2 : tokens_own + 3],
            blank(2 * PAD - 3),
            low[2:],
            context,
            high[1:],
            blank(PAD - 1),
        ]
    )
    near, xs, bc, z_act, running, dt, gate = front(
        jnp.stack([place == 0, place == count - 1]).astype(jnp.int32),
        rows,
        mods,
        norm_gain[None],
        jnp.concatenate([w_dt[0], w_dt[1]], axis=1).T,
        jnp.concatenate([conv_x, conv_b, conv_c], axis=1),
        decay_rate.reshape(1, 2 * heads),
        jnp.concatenate([decay_extra, decay_extra], axis=1),
        w_x,
        w_gate,
        jnp.concatenate([w_b, w_c], axis=1),
        lax.axis_size(NEAR),
    )
    bmat, cmat = bc[:, :STATE], bc[:, STATE:]
    entry = entry_states(near, heads)

    affinity = lax.dot_general(cmat, bmat, (((1,), (1,)), ((), ())), preferred_element_type=F32)
    i = jnp.arange(tokens)
    lower = i[:, None] >= i[None, :]
    upper = i[:, None] <= i[None, :]
    parts = []
    for h in range(heads):
        weights = jnp.zeros((tokens, tokens), F32)
        for d, mask in ((0, lower), (1, upper)):
            col = d * heads + h
            gap = running[:, col][:, None] - running[:, col][None, :]
            mixing = jnp.where(mask, jnp.exp(jnp.where(mask, gap, 0.0)), 0.0)
            weights = weights + mixing * dt[:, col][None, :]
        weights = (affinity * weights).astype(BF16)
        parts.append(jnp.dot(weights, xs[:, h * HEAD_DIM : (h + 1) * HEAD_DIM], preferred_element_type=F32))
    y = jnp.concatenate(parts, axis=1)
    flat = entry.transpose(1, 0, 2).reshape(STATE, heads * 128)
    carried = jnp.dot(cmat, flat, preferred_element_type=F32) * wide(jnp.exp(running))
    carried = carried.reshape(tokens, heads, 2, HEAD_DIM)
    y = y + (carried[:, :, 0] + carried[:, :, 1]).reshape(tokens, heads * HEAD_DIM)
    gated = y * z_act
    mean_square = jnp.mean(gated * gated, axis=1, keepdims=True)
    normed = (gated * lax.rsqrt(mean_square + GROUP_EPS) * out_gain.astype(F32)).astype(BF16)
    tp_count = lax.axis_size("tp")
    stacked = normed.reshape(tp_count, tokens // tp_count, head_cols)
    return last(exchange(stacked, "tp"), latent, gate, w_out)


def solution(mesh):
    sp, tp, dp = (mesh.shape[a] for a in ("sp", "tp", "dp"))
    inner = Mesh(np.asarray(mesh.devices).reshape(sp // 8, 4, 2, tp, dp), (*SP, "tp", "dp"))
    in_specs = (
        P(("dp", *SP, "tp"), None),
        P("dp"),
        P(("dp", *SP), None),
        P(),
        P((*SP, "tp"), None),
        P(),
        P(None, "tp"),
        P(None, "tp"),
        P(None, "tp"),
        P(None, "tp"),
        P(None, None, "tp"),
        P(None, "tp"),
        P(None, "tp"),
        P(None, "tp"),
        P(None, "tp"),
        P(("dp", *SP), "tp"),
        P("tp"),
        P(),
    )
    out_specs = P(("dp", *SP, "tp"), None)
    return jax.shard_map(program, mesh=inner, in_specs=in_specs, out_specs=out_specs, check_vma=False)
```

```python
import jax
import jax.numpy as jnp
import numpy as np
from jax import lax
from jax.experimental import pallas as pl
from jax.experimental.pallas import tpu as pltpu
from jax.sharding import Mesh
from jax.sharding import PartitionSpec as P


HEAD_DIM = 64
STATE = 64
ROW_EPS = 1e-06
GROUP_EPS = 1e-05
HIGHEST = lax.Precision.HIGHEST
F32 = jnp.float32
BF16 = jnp.bfloat16
PAD = 8

SP = ("za", "zb", "zc")
NEAR = ("zb", "zc")
MOD_NEAR = ("zc", "tp")
MOD_FAR = ("za", "zb")


def exchange(x, axis):
    return lax.all_to_all(x, axis, 0, 0, tiled=True)


def share(x, axis):
    n = lax.axis_size(axis)
    full = jnp.broadcast_to(x[None], (n, *x.shape)).reshape(n * x.shape[0], *x.shape[1:])
    return exchange(full, axis).reshape(n, *x.shape)


def ring_rows(x):
    n = lax.axis_size("tp")
    moved = [x] + [lax.ppermute(x, "tp", [(i, (i + k) % n) for i in range(n)]) for k in range(1, n)]
    moved = jnp.stack(moved)
    place = lax.axis_index("tp")
    return jnp.stack([lax.dynamic_index_in_dim(moved, (place - t) % n, 0, False) for t in range(n)])


def split_hi_lo(x):
    hi = lax.reduce_precision(x, 8, 7)
    return hi, x - hi


def whole(shape):
    return pl.BlockSpec(shape, lambda i: (0,) * len(shape))


def silu(v):
    return v / (1.0 + jnp.exp(-v))


def partial_kernel(first, cond, context_cond, modulation, out):
    share_rows, cols = modulation.shape
    width = cols // 3
    at = first[0] + lax.broadcasted_iota(jnp.int32, (share_rows, width), 0)
    pick = jnp.where(lax.broadcasted_iota(jnp.int32, (share_rows, width), 1) == at, 1.0, 0.0).astype(BF16)
    table = modulation[...]
    cut = width // (out.shape[0] // 5)
    for source, kinds in ((0, (0, 1, 2)), (1, (0, 1))):
        v = (cond, context_cond)[source][...].astype(F32).reshape(1, width)
        row = silu(v).astype(BF16)
        own = lax.dot_general(row, pick, (((1,), (1,)), ((), ())), preferred_element_type=F32).astype(BF16)
        sums = jnp.dot(own, table, preferred_element_type=F32)
        for kind in kinds:
            for n in range(width // cut):
                for r in range(2):
                    at = kind * width + n * cut + r * 128
                    out[n * 5 + 3 * source + kind, r : r + 1, :] = sums[0:1, at : at + 128]


def partial_mods(first, cond, context_cond, modulation, n):
    return pl.pallas_call(
        partial_kernel,
        grid=(1,),
        out_shape=jax.ShapeDtypeStruct((n * 5, 2, 128), F32),
        in_specs=[pl.BlockSpec(memory_space=pltpu.SMEM)] + [whole(v.shape) for v in (cond, context_cond, modulation)],
        out_specs=whole((n * 5, 2, 128)),
        name="partial_mods",
    )(first.astype(jnp.int32).reshape(1), cond, context_cond, modulation)


def mod_vectors(cond, context_cond, modulation, own_rows):
    share_rows = modulation.shape[0]
    width = modulation.shape[1] // 3
    n = lax.axis_size(MOD_NEAR)
    cut = width // n
    pairs = 5 * cut // 256
    first = lax.axis_index((*SP, "tp")) * share_rows
    part = partial_mods(first, cond, context_cond, modulation, n)
    part = jnp.sum(exchange(part, MOD_NEAR).reshape(n, pairs, 2, 128), axis=0)
    far = share(part, MOD_FAR)
    gathered = ring_rows(own_rows)
    full = share(jnp.sum(far, axis=0), MOD_NEAR)
    return full.reshape(n, 5, cut).transpose(1, 0, 2).reshape(5, width), gathered


def modulated_norm(rows, norm_gain, shift_row, scale_row):
    values = rows.astype(F32)
    normed = values * lax.rsqrt(jnp.mean(values * values, axis=-1, keepdims=True) + ROW_EPS)
    return (normed * norm_gain.astype(F32) * (1.0 + scale_row) + shift_row).astype(BF16)


def conv(values, taps, first, length):
    total = jnp.zeros((length, values.shape[1]), F32)
    for k in range(4):
        total = total + taps[k].astype(F32) * values[first + k : first + k + length]
    return jax.nn.silu(total).astype(BF16)


def wide(v):
    heads = v.shape[1] // 2
    v = v.reshape(v.shape[0], 2, heads).transpose(0, 2, 1)
    return jnp.repeat(v, HEAD_DIM, axis=2).reshape(v.shape[0], heads * 2 * HEAD_DIM)


def twice(x):
    heads = x.shape[1] // HEAD_DIM
    v = x.reshape(x.shape[0], heads, 1, HEAD_DIM)
    return jnp.broadcast_to(v, (x.shape[0], heads, 2, HEAD_DIM)).reshape(x.shape[0], heads * 2 * HEAD_DIM)


def running_sums(log_decay):
    length = log_decay.shape[0]
    heads = log_decay.shape[1] // 2
    i = jnp.arange(length)
    low = (i[:, None] >= i[None, :]).astype(F32)
    forward = jnp.dot(low, log_decay[:, :heads], precision=HIGHEST)
    backward = jnp.dot(low.T, log_decay[:, heads:], precision=HIGHEST)
    return jnp.concatenate([forward, backward], axis=1)


def end_states(xs, bmat, dt, running, total):
    weights = wide(jnp.exp(total - running) * dt)
    weighted = (twice(xs).astype(F32) * weights).astype(BF16)
    return lax.dot_general(bmat, weighted, (((0,), (0,)), ((), ())), preferred_element_type=F32)


def entry_sums(states, totals, f_lane):
    n = states.shape[0]
    m = lax.broadcasted_iota(jnp.int32, (n + 1, n, n, 1), 0)
    k = lax.broadcasted_iota(jnp.int32, (n + 1, n, n, 1), 1)
    j = lax.broadcasted_iota(jnp.int32, (n + 1, n, n, 1), 2)
    mb = jnp.where(m == n, -1, m)
    between = jnp.where(f_lane, (j > k) & (j < m), (j < k) & (j > mb))
    gap = jnp.sum(jnp.where(between, totals[None, None], 0.0), axis=2)
    ahead = jnp.where(f_lane, k[:, :, 0] < m[:, :, 0], k[:, :, 0] > mb[:, :, 0])
    factor = jnp.where(ahead, jnp.exp(gap), 0.0)
    sums = jnp.sum(factor[:, :, None] * states[None], axis=1)
    to_m = jnp.sum(jnp.where(ahead, totals[None], 0.0), axis=1)
    return sums, to_m


def entry_states(ctx_state, ctx_total, lat_state, lat_total):
    heads = ctx_total.shape[1] // 2
    n = lax.axis_size(NEAR)
    half = heads * STATE // n

    def pieces(state):
        v = state.reshape(STATE // half, half, heads, 128).transpose(2, 0, 1, 3)
        return v.reshape(n, half, 128)

    decays = []
    for total in (ctx_total, lat_total):
        w = jnp.repeat(wide(total).reshape(heads, 1, 128), STATE // half, axis=0)
        decays += list(split_hi_lo(w))
    decays.append(jnp.zeros((n, 4, 128), F32))
    near = jnp.concatenate([pieces(ctx_state), pieces(lat_state), *decays], axis=1).astype(BF16)
    near = exchange(near, NEAR).astype(F32)
    f_lane = lax.broadcasted_iota(jnp.int32, (1, 128), 1) < HEAD_DIM
    ctx_t = near[:, 2 * half] + near[:, 2 * half + 1]
    lat_t = near[:, 2 * half + 2] + near[:, 2 * half + 3]
    ctx_sums, ctx_to = entry_sums(near[:, :half], ctx_t, f_lane)
    lat_sums, lat_to = entry_sums(near[:, half : 2 * half], lat_t, f_lane)
    far = jnp.concatenate(
        [ctx_sums[n], lat_sums[n], *split_hi_lo(ctx_to[n:]), *split_hi_lo(lat_to[n:]), jnp.zeros((4, 128), F32)], axis=0
    ).astype(BF16)
    far = share(far, "za").astype(F32)
    count = far.shape[0]
    start, _ = entry_sums(far[:, :half], far[:, 2 * half] + far[:, 2 * half + 1], f_lane)
    group, group_to = entry_sums(far[:, half : 2 * half], far[:, 2 * half + 2] + far[:, 2 * half + 3], f_lane)
    mine = (jnp.arange(count + 1) == lax.axis_index("za")).astype(F32)
    group = jnp.sum(mine[:, None, None] * group, axis=0)
    group_to = jnp.sum(mine[:, None] * group_to, axis=0)
    entry = jnp.exp(group_to) * start[count] + group
    back = (jnp.exp(lat_to[:n, None]) * entry + lat_sums[:n]).astype(BF16)
    back = exchange(back, NEAR)
    return back.reshape(heads, STATE, 128)


def program(
    latent,
    cond,
    context,
    context_cond,
    modulation,
    norm_gain,
    w_x,
    w_gate,
    w_b,
    w_c,
    w_dt,
    conv_x,
    conv_b,
    conv_c,
    decay_rate,
    decay_extra,
    out_gain,
    w_out,
):
    heads = w_dt.shape[2]
    head_cols = w_x.shape[1]
    tokens = decay_extra.shape[0]
    ctx_tokens = context.shape[0]
    count = lax.axis_size(SP)
    place = lax.axis_index(SP)
    up = [(i, i + 1) for i in range(count - 1)]
    down = [(i + 1, i) for i in range(count - 1)]
    low = lax.ppermute(jnp.concatenate([latent[-PAD:], context[-PAD:]]), SP, up)
    high = lax.ppermute(jnp.concatenate([latent[:PAD], context[:PAD]]), SP, down)
    own = jnp.concatenate([latent, low[:PAD], high[:PAD]])
    context_rows = jnp.concatenate([low[PAD:], context, high[PAD:]])
    mods, gathered = mod_vectors(cond, context_cond, modulation, own)
    tokens_own = latent.shape[0]
    latent_rows = jnp.concatenate(
        [
            gathered[-1, tokens_own : tokens_own + PAD],
            gathered[:, :tokens_own].reshape(tokens, latent.shape[1]),
            gathered[0, tokens_own + PAD :],
        ]
    )

    lat_len = tokens + 2 * PAD
    hidden = jnp.concatenate(
        [
            modulated_norm(latent_rows, norm_gain, mods[0], mods[1]),
            modulated_norm(context_rows, norm_gain, mods[3], mods[4]),
        ]
    )
    row = jnp.arange(hidden.shape[0])
    first = (row < PAD) | ((row >= lat_len) & (row < lat_len + PAD))
    last = ((row >= lat_len - PAD) & (row < lat_len)) | (row >= hidden.shape[0] - PAD)
    outside = (first & (place == 0)) | (last & (place == count - 1))
    inner = hidden[PAD : PAD + tokens]

    def project(rows, weight):
        return jnp.dot(rows, weight, preferred_element_type=F32).astype(BF16)

    p_x = jnp.where(outside[:, None], 0.0, project(hidden, w_x).astype(F32))
    p_b = jnp.where(outside[:, None], 0.0, project(hidden, w_b).astype(F32))
    p_c = jnp.where(outside[:lat_len, None], 0.0, project(hidden[:lat_len], w_c).astype(F32))
    p_dt = jax.nn.softplus(project(hidden, jnp.concatenate([w_dt[0], w_dt[1]], axis=1)).astype(F32))
    z = project(inner, w_gate).astype(F32)

    off = PAD - 2
    xs = conv(p_x, conv_x, off, tokens)
    bmat = conv(p_b, conv_b, off, tokens)
    cmat = conv(p_c, conv_c, off, tokens)
    ctx_xs = conv(p_x, conv_x, lat_len + off, ctx_tokens)
    ctx_b = conv(p_b, conv_b, lat_len + off, ctx_tokens)
    dt = p_dt[PAD : PAD + tokens]
    ctx_dt = p_dt[lat_len + PAD : lat_len + PAD + ctx_tokens]
    rate = decay_rate.reshape(1, 2 * heads)
    log_decay = -rate * dt + jnp.concatenate([decay_extra, decay_extra], axis=1)
    ctx_log_decay = -rate * ctx_dt
    running = running_sums(log_decay)
    ctx_running = running_sums(ctx_log_decay)
    total = jnp.sum(log_decay, axis=0, keepdims=True)
    ctx_total = jnp.sum(ctx_log_decay, axis=0, keepdims=True)
    entry = entry_states(
        end_states(ctx_xs, ctx_b, ctx_dt, ctx_running, ctx_total),
        ctx_total,
        end_states(xs, bmat, dt, running, total),
        total,
    )

    affinity = lax.dot_general(cmat, bmat, (((1,), (1,)), ((), ())), preferred_element_type=F32)
    i = jnp.arange(tokens)
    lower = i[:, None] >= i[None, :]
    upper = i[:, None] <= i[None, :]
    parts = []
    for h in range(heads):
        weights = jnp.zeros((tokens, tokens), F32)
        for d, mask in ((0, lower), (1, upper)):
            col = d * heads + h
            gap = running[:, col][:, None] - running[:, col][None, :]
            mixing = jnp.where(mask, jnp.exp(jnp.where(mask, gap, 0.0)), 0.0)
            weights = weights + mixing * dt[:, col][None, :]
        weights = (affinity * weights).astype(BF16)
        parts.append(jnp.dot(weights, xs[:, h * HEAD_DIM : (h + 1) * HEAD_DIM], preferred_element_type=F32))
    y = jnp.concatenate(parts, axis=1)
    flat = entry.transpose(1, 0, 2).reshape(STATE, heads * 128)
    carried = jnp.dot(cmat, flat, preferred_element_type=F32) * wide(jnp.exp(running))
    carried = carried.reshape(tokens, heads, 2, HEAD_DIM)
    y = y + (carried[:, :, 0] + carried[:, :, 1]).reshape(tokens, heads * HEAD_DIM)
    gated = y * jax.nn.silu(z)
    mean_square = jnp.mean(gated * gated, axis=1, keepdims=True)
    normed = (gated * lax.rsqrt(mean_square + GROUP_EPS) * out_gain.astype(F32)).astype(BF16)
    tp_count = lax.axis_size("tp")
    stacked = normed.reshape(tp_count, tokens // tp_count, head_cols)
    full = lax.all_to_all(stacked, "tp", split_axis=0, concat_axis=2, tiled=True)[0]
    branch = jnp.dot(full, w_out, preferred_element_type=F32)
    return (latent.astype(F32) + mods[2] * branch).astype(BF16)


def solution(mesh):
    sp, tp, dp = (mesh.shape[a] for a in ("sp", "tp", "dp"))
    inner = Mesh(np.asarray(mesh.devices).reshape(sp // 8, 4, 2, tp, dp), (*SP, "tp", "dp"))
    in_specs = (
        P(("dp", *SP, "tp"), None),
        P("dp"),
        P(("dp", *SP), None),
        P(),
        P((*SP, "tp"), None),
        P(),
        P(None, "tp"),
        P(None, "tp"),
        P(None, "tp"),
        P(None, "tp"),
        P(None, None, "tp"),
        P(None, "tp"),
        P(None, "tp"),
        P(None, "tp"),
        P(None, "tp"),
        P(("dp", *SP), "tp"),
        P("tp"),
        P(),
    )
    out_specs = P(("dp", *SP, "tp"), None)
    return jax.shard_map(program, mesh=inner, in_specs=in_specs, out_specs=out_specs, check_vma=False)
```

```python
import jax
import jax.numpy as jnp
import numpy as np
from jax import lax
from jax.experimental import pallas as pl
from jax.experimental.pallas import tpu as pltpu
from jax.sharding import Mesh
from jax.sharding import PartitionSpec as P


HEAD_DIM = 64
STATE = 64
ROW_EPS = 1e-06
GROUP_EPS = 1e-05
HIGHEST = lax.Precision.HIGHEST
F32 = jnp.float32
BF16 = jnp.bfloat16
PAD = 8

SP = ("za", "zb", "zc")
NEAR = ("zb", "zc")
MOD_NEAR = ("zc", "tp")
MOD_FAR = ("za", "zb")


def exchange(x, axis):
    return lax.all_to_all(x, axis, 0, 0, tiled=True)


def share(x, axis):
    n = lax.axis_size(axis)
    full = jnp.broadcast_to(x[None], (n, *x.shape)).reshape(n * x.shape[0], *x.shape[1:])
    return exchange(full, axis).reshape(n, *x.shape)


def ring_rows(x):
    n = lax.axis_size("tp")
    moved = [x] + [lax.ppermute(x, "tp", [(i, (i + k) % n) for i in range(n)]) for k in range(1, n)]
    moved = jnp.stack(moved)
    place = lax.axis_index("tp")
    return jnp.stack([lax.dynamic_index_in_dim(moved, (place - t) % n, 0, False) for t in range(n)])


def split_hi_lo(x):
    hi = lax.reduce_precision(x, 8, 7)
    return hi, x - hi


def whole(shape):
    return pl.BlockSpec(shape, lambda i: (0,) * len(shape))


def silu(v):
    return v / (1.0 + jnp.exp(-v))


def partial_kernel(first, cond, context_cond, modulation, out):
    share_rows, cols = modulation.shape
    width = cols // 3
    at = first[0] + lax.broadcasted_iota(jnp.int32, (share_rows, width), 0)
    pick = jnp.where(lax.broadcasted_iota(jnp.int32, (share_rows, width), 1) == at, 1.0, 0.0).astype(BF16)
    table = modulation[...]
    cut = width // (out.shape[0] // 5)
    for source, kinds in ((0, (0, 1, 2)), (1, (0, 1))):
        v = (cond, context_cond)[source][...].astype(F32).reshape(1, width)
        row = silu(v).astype(BF16)
        own = lax.dot_general(row, pick, (((1,), (1,)), ((), ())), preferred_element_type=F32).astype(BF16)
        sums = jnp.dot(own, table, preferred_element_type=F32)
        for kind in kinds:
            for n in range(width // cut):
                for r in range(2):
                    at = kind * width + n * cut + r * 128
                    out[n * 5 + 3 * source + kind, r : r + 1, :] = sums[0:1, at : at + 128]


def partial_mods(first, cond, context_cond, modulation, n):
    return pl.pallas_call(
        partial_kernel,
        grid=(1,),
        out_shape=jax.ShapeDtypeStruct((n * 5, 2, 128), F32),
        in_specs=[pl.BlockSpec(memory_space=pltpu.SMEM)] + [whole(v.shape) for v in (cond, context_cond, modulation)],
        out_specs=whole((n * 5, 2, 128)),
        name="partial_mods",
    )(first.astype(jnp.int32).reshape(1), cond, context_cond, modulation)


def mod_vectors(cond, context_cond, modulation, own_rows, held):
    share_rows = modulation.shape[0]
    width = modulation.shape[1] // 3
    n = lax.axis_size(MOD_NEAR)
    cut = width // n
    pairs = 5 * cut // 256
    first = lax.axis_index((*SP, "tp")) * share_rows
    part = partial_mods(first, cond, context_cond, modulation, n)
    part = jnp.sum(exchange(part, MOD_NEAR).reshape(n, pairs, 2, 128), axis=0)
    part, held = lax.optimization_barrier((part, held))
    far = share(part, MOD_FAR)
    gathered = ring_rows(own_rows)
    full = share(jnp.sum(far, axis=0), MOD_NEAR)
    return full.reshape(n, 5, cut).transpose(1, 0, 2).reshape(5, width), gathered, held


def modulated_norm(rows, norm_gain, shift_row, scale_row):
    values = rows.astype(F32)
    normed = values * lax.rsqrt(jnp.mean(values * values, axis=-1, keepdims=True) + ROW_EPS)
    return (normed * norm_gain.astype(F32) * (1.0 + scale_row) + shift_row).astype(BF16)


def conv(values, taps, first, length):
    total = jnp.zeros((length, values.shape[1]), F32)
    for k in range(4):
        total = total + taps[k].astype(F32) * values[first + k : first + k + length]
    return jax.nn.silu(total).astype(BF16)


def wide(v):
    heads = v.shape[1] // 2
    v = v.reshape(v.shape[0], 2, heads).transpose(0, 2, 1)
    return jnp.repeat(v, HEAD_DIM, axis=2).reshape(v.shape[0], heads * 2 * HEAD_DIM)


def twice(x):
    heads = x.shape[1] // HEAD_DIM
    v = x.reshape(x.shape[0], heads, 1, HEAD_DIM)
    return jnp.broadcast_to(v, (x.shape[0], heads, 2, HEAD_DIM)).reshape(x.shape[0], heads * 2 * HEAD_DIM)


def running_sums(log_decay):
    length = log_decay.shape[0]
    heads = log_decay.shape[1] // 2
    i = jnp.arange(length)
    low = (i[:, None] >= i[None, :]).astype(F32)
    forward = jnp.dot(low, log_decay[:, :heads], precision=HIGHEST)
    backward = jnp.dot(low.T, log_decay[:, heads:], precision=HIGHEST)
    return jnp.concatenate([forward, backward], axis=1)


def end_states(xs, bmat, dt, running, total):
    weights = wide(jnp.exp(total - running) * dt)
    weighted = (twice(xs).astype(F32) * weights).astype(BF16)
    return lax.dot_general(bmat, weighted, (((0,), (0,)), ((), ())), preferred_element_type=F32)


def entry_sums(states, totals, f_lane):
    n = states.shape[0]
    m = lax.broadcasted_iota(jnp.int32, (n + 1, n, n, 1), 0)
    k = lax.broadcasted_iota(jnp.int32, (n + 1, n, n, 1), 1)
    j = lax.broadcasted_iota(jnp.int32, (n + 1, n, n, 1), 2)
    mb = jnp.where(m == n, -1, m)
    between = jnp.where(f_lane, (j > k) & (j < m), (j < k) & (j > mb))
    gap = jnp.sum(jnp.where(between, totals[None, None], 0.0), axis=2)
    ahead = jnp.where(f_lane, k[:, :, 0] < m[:, :, 0], k[:, :, 0] > mb[:, :, 0])
    factor = jnp.where(ahead, jnp.exp(gap), 0.0)
    sums = jnp.sum(factor[:, :, None] * states[None], axis=1)
    to_m = jnp.sum(jnp.where(ahead, totals[None], 0.0), axis=1)
    return sums, to_m


def entry_states(ctx_state, ctx_total, lat_state, lat_total):
    heads = ctx_total.shape[1] // 2
    n = lax.axis_size(NEAR)
    half = heads * STATE // n

    def pieces(state):
        v = state.reshape(STATE // half, half, heads, 128).transpose(2, 0, 1, 3)
        return v.reshape(n, half, 128)

    decays = []
    for total in (ctx_total, lat_total):
        w = jnp.repeat(wide(total).reshape(heads, 1, 128), STATE // half, axis=0)
        decays += list(split_hi_lo(w))
    decays.append(jnp.zeros((n, 4, 128), F32))
    near = jnp.concatenate([pieces(ctx_state), pieces(lat_state), *decays], axis=1).astype(BF16)
    near = exchange(near, NEAR).astype(F32)
    f_lane = lax.broadcasted_iota(jnp.int32, (1, 128), 1) < HEAD_DIM
    ctx_t = near[:, 2 * half] + near[:, 2 * half + 1]
    lat_t = near[:, 2 * half + 2] + near[:, 2 * half + 3]
    ctx_sums, ctx_to = entry_sums(near[:, :half], ctx_t, f_lane)
    lat_sums, lat_to = entry_sums(near[:, half : 2 * half], lat_t, f_lane)
    far = jnp.concatenate(
        [ctx_sums[n], lat_sums[n], *split_hi_lo(ctx_to[n:]), *split_hi_lo(lat_to[n:]), jnp.zeros((4, 128), F32)], axis=0
    ).astype(BF16)
    far = share(far, "za").astype(F32)
    count = far.shape[0]
    start, _ = entry_sums(far[:, :half], far[:, 2 * half] + far[:, 2 * half + 1], f_lane)
    group, group_to = entry_sums(far[:, half : 2 * half], far[:, 2 * half + 2] + far[:, 2 * half + 3], f_lane)
    mine = (jnp.arange(count + 1) == lax.axis_index("za")).astype(F32)
    group = jnp.sum(mine[:, None, None] * group, axis=0)
    group_to = jnp.sum(mine[:, None] * group_to, axis=0)
    entry = jnp.exp(group_to) * start[count] + group
    back = (jnp.exp(lat_to[:n, None]) * entry + lat_sums[:n]).astype(BF16)
    back = exchange(back, NEAR)
    return back.reshape(heads, STATE, 128)


def program(
    latent,
    cond,
    context,
    context_cond,
    modulation,
    norm_gain,
    w_x,
    w_gate,
    w_b,
    w_c,
    w_dt,
    conv_x,
    conv_b,
    conv_c,
    decay_rate,
    decay_extra,
    out_gain,
    w_out,
):
    heads = w_dt.shape[2]
    head_cols = w_x.shape[1]
    tokens = decay_extra.shape[0]
    ctx_tokens = context.shape[0]
    count = lax.axis_size(SP)
    place = lax.axis_index(SP)
    up = [(i, i + 1) for i in range(count - 1)]
    down = [(i + 1, i) for i in range(count - 1)]
    low = lax.ppermute(jnp.concatenate([latent[-PAD:], context[-PAD:]]), SP, up)
    high = lax.ppermute(jnp.concatenate([latent[:PAD], context[:PAD]]), SP, down)
    own = jnp.concatenate([latent, low[:PAD], high[:PAD]])
    context_rows = jnp.concatenate([low[PAD:], context, high[PAD:]])
    held = (conv_x, conv_b, conv_c, decay_rate, decay_extra, norm_gain, w_dt, out_gain)
    mods, gathered, held = mod_vectors(cond, context_cond, modulation, own, held)
    conv_x, conv_b, conv_c, decay_rate, decay_extra, norm_gain, w_dt, out_gain = held
    tokens_own = latent.shape[0]
    latent_rows = jnp.concatenate(
        [
            gathered[-1, tokens_own : tokens_own + PAD],
            gathered[:, :tokens_own].reshape(tokens, latent.shape[1]),
            gathered[0, tokens_own + PAD :],
        ]
    )

    lat_len = tokens + 2 * PAD
    hidden = jnp.concatenate(
        [
            modulated_norm(latent_rows, norm_gain, mods[0], mods[1]),
            modulated_norm(context_rows, norm_gain, mods[3], mods[4]),
        ]
    )
    row = jnp.arange(hidden.shape[0])
    first = (row < PAD) | ((row >= lat_len) & (row < lat_len + PAD))
    last = ((row >= lat_len - PAD) & (row < lat_len)) | (row >= hidden.shape[0] - PAD)
    outside = (first & (place == 0)) | (last & (place == count - 1))
    inner = hidden[PAD : PAD + tokens]

    def project(rows, weight):
        return jnp.dot(rows, weight, preferred_element_type=F32).astype(BF16)

    p_x = jnp.where(outside[:, None], 0.0, project(hidden, w_x).astype(F32))
    p_b = jnp.where(outside[:, None], 0.0, project(hidden, w_b).astype(F32))
    p_c = jnp.where(outside[:lat_len, None], 0.0, project(hidden[:lat_len], w_c).astype(F32))
    p_dt = jax.nn.softplus(project(hidden, jnp.concatenate([w_dt[0], w_dt[1]], axis=1)).astype(F32))
    z = project(inner, w_gate).astype(F32)

    off = PAD - 2
    xs = conv(p_x, conv_x, off, tokens)
    bmat = conv(p_b, conv_b, off, tokens)
    cmat = conv(p_c, conv_c, off, tokens)
    ctx_xs = conv(p_x, conv_x, lat_len + off, ctx_tokens)
    ctx_b = conv(p_b, conv_b, lat_len + off, ctx_tokens)
    dt = p_dt[PAD : PAD + tokens]
    ctx_dt = p_dt[lat_len + PAD : lat_len + PAD + ctx_tokens]
    rate = decay_rate.reshape(1, 2 * heads)
    log_decay = -rate * dt + jnp.concatenate([decay_extra, decay_extra], axis=1)
    ctx_log_decay = -rate * ctx_dt
    running = running_sums(log_decay)
    ctx_running = running_sums(ctx_log_decay)
    total = jnp.sum(log_decay, axis=0, keepdims=True)
    ctx_total = jnp.sum(ctx_log_decay, axis=0, keepdims=True)
    entry = entry_states(
        end_states(ctx_xs, ctx_b, ctx_dt, ctx_running, ctx_total),
        ctx_total,
        end_states(xs, bmat, dt, running, total),
        total,
    )

    affinity = lax.dot_general(cmat, bmat, (((1,), (1,)), ((), ())), preferred_element_type=F32)
    i = jnp.arange(tokens)
    lower = i[:, None] >= i[None, :]
    upper = i[:, None] <= i[None, :]
    parts = []
    for h in range(heads):
        weights = jnp.zeros((tokens, tokens), F32)
        for d, mask in ((0, lower), (1, upper)):
            col = d * heads + h
            gap = running[:, col][:, None] - running[:, col][None, :]
            mixing = jnp.where(mask, jnp.exp(jnp.where(mask, gap, 0.0)), 0.0)
            weights = weights + mixing * dt[:, col][None, :]
        weights = (affinity * weights).astype(BF16)
        parts.append(jnp.dot(weights, xs[:, h * HEAD_DIM : (h + 1) * HEAD_DIM], preferred_element_type=F32))
    y = jnp.concatenate(parts, axis=1)
    flat = entry.transpose(1, 0, 2).reshape(STATE, heads * 128)
    carried = jnp.dot(cmat, flat, preferred_element_type=F32) * wide(jnp.exp(running))
    carried = carried.reshape(tokens, heads, 2, HEAD_DIM)
    y = y + (carried[:, :, 0] + carried[:, :, 1]).reshape(tokens, heads * HEAD_DIM)
    gated = y * jax.nn.silu(z)
    mean_square = jnp.mean(gated * gated, axis=1, keepdims=True)
    normed = (gated * lax.rsqrt(mean_square + GROUP_EPS) * out_gain.astype(F32)).astype(BF16)
    tp_count = lax.axis_size("tp")
    stacked = normed.reshape(tp_count, tokens // tp_count, head_cols)
    full = lax.all_to_all(stacked, "tp", split_axis=0, concat_axis=2, tiled=True)[0]
    branch = jnp.dot(full, w_out, preferred_element_type=F32)
    return (latent.astype(F32) + mods[2] * branch).astype(BF16)


def solution(mesh):
    sp, tp, dp = (mesh.shape[a] for a in ("sp", "tp", "dp"))
    inner = Mesh(np.asarray(mesh.devices).reshape(sp // 8, 4, 2, tp, dp), (*SP, "tp", "dp"))
    in_specs = (
        P(("dp", *SP, "tp"), None),
        P("dp"),
        P(("dp", *SP), None),
        P(),
        P((*SP, "tp"), None),
        P(),
        P(None, "tp"),
        P(None, "tp"),
        P(None, "tp"),
        P(None, "tp"),
        P(None, None, "tp"),
        P(None, "tp"),
        P(None, "tp"),
        P(None, "tp"),
        P(None, "tp"),
        P(("dp", *SP), "tp"),
        P("tp"),
        P(),
    )
    out_specs = P(("dp", *SP, "tp"), None)
    return jax.shard_map(program, mesh=inner, in_specs=in_specs, out_specs=out_specs, check_vma=False)
```

```python
import jax
import jax.numpy as jnp
import numpy as np
from jax import lax
from jax.experimental import pallas as pl
from jax.experimental.pallas import tpu as pltpu
from jax.sharding import Mesh
from jax.sharding import PartitionSpec as P


HEAD_DIM = 64
STATE = 64
ROW_EPS = 1e-06
GROUP_EPS = 1e-05
HIGHEST = lax.Precision.HIGHEST
F32 = jnp.float32
BF16 = jnp.bfloat16
PAD = 8

SP = ("za", "zb", "zc")
NEAR = ("zb", "zc")
MOD_NEAR = ("zc", "tp")
MOD_FAR = ("za", "zb")


def exchange(x, axis):
    return lax.all_to_all(x, axis, 0, 0, tiled=True)


def share(x, axis):
    n = lax.axis_size(axis)
    full = jnp.broadcast_to(x[None], (n, *x.shape)).reshape(n * x.shape[0], *x.shape[1:])
    return exchange(full, axis).reshape(n, *x.shape)


def ring_rows(x):
    n = lax.axis_size("tp")
    moved = [x] + [lax.ppermute(x, "tp", [(i, (i + k) % n) for i in range(n)]) for k in range(1, n)]
    moved = jnp.stack(moved)
    place = lax.axis_index("tp")
    return jnp.stack([lax.dynamic_index_in_dim(moved, (place - t) % n, 0, False) for t in range(n)])


def split_hi_lo(x):
    hi = lax.reduce_precision(x, 8, 7)
    return hi, x - hi


def whole(shape):
    return pl.BlockSpec(shape, lambda i: (0,) * len(shape))


def silu(v):
    return v / (1.0 + jnp.exp(-v))


def partial_kernel(first, cond, context_cond, modulation, out):
    share_rows, cols = modulation.shape
    width = cols // 3
    at = first[0] + lax.broadcasted_iota(jnp.int32, (share_rows, width), 0)
    pick = jnp.where(lax.broadcasted_iota(jnp.int32, (share_rows, width), 1) == at, 1.0, 0.0).astype(BF16)
    table = modulation[...]
    cut = width // (out.shape[0] // 5)
    for source, kinds in ((0, (0, 1, 2)), (1, (0, 1))):
        v = (cond, context_cond)[source][...].astype(F32).reshape(1, width)
        row = silu(v).astype(BF16)
        own = lax.dot_general(row, pick, (((1,), (1,)), ((), ())), preferred_element_type=F32).astype(BF16)
        sums = jnp.dot(own, table, preferred_element_type=F32)
        for kind in kinds:
            for n in range(width // cut):
                for r in range(2):
                    at = kind * width + n * cut + r * 128
                    out[n * 5 + 3 * source + kind, r : r + 1, :] = sums[0:1, at : at + 128]


def partial_mods(first, cond, context_cond, modulation, n):
    return pl.pallas_call(
        partial_kernel,
        grid=(1,),
        out_shape=jax.ShapeDtypeStruct((n * 5, 2, 128), F32),
        in_specs=[pl.BlockSpec(memory_space=pltpu.SMEM)] + [whole(v.shape) for v in (cond, context_cond, modulation)],
        out_specs=whole((n * 5, 2, 128)),
        name="partial_mods",
    )(first.astype(jnp.int32).reshape(1), cond, context_cond, modulation)


def mod_vectors(cond, context_cond, modulation, own_rows, held):
    share_rows = modulation.shape[0]
    width = modulation.shape[1] // 3
    n = lax.axis_size(MOD_NEAR)
    cut = width // n
    pairs = 5 * cut // 256
    first = lax.axis_index((*SP, "tp")) * share_rows
    part = partial_mods(first, cond, context_cond, modulation, n)
    part = jnp.sum(exchange(part, MOD_NEAR).reshape(n, pairs, 2, 128), axis=0)
    part, held = lax.optimization_barrier((part, held))
    far = share(part, MOD_FAR)
    gathered = ring_rows(own_rows)
    full = share(jnp.sum(far, axis=0), MOD_NEAR)
    return full.reshape(n, 5, cut).transpose(1, 0, 2).reshape(5, width), gathered, held


def modulated_norm(rows, norm_gain, shift_row, scale_row):
    values = rows.astype(F32)
    normed = values * lax.rsqrt(jnp.mean(values * values, axis=-1, keepdims=True) + ROW_EPS)
    return (normed * norm_gain.astype(F32) * (1.0 + scale_row) + shift_row).astype(BF16)


def conv(values, taps, first, length):
    total = jnp.zeros((length, values.shape[1]), F32)
    for k in range(4):
        total = total + taps[k].astype(F32) * values[first + k : first + k + length]
    return jax.nn.silu(total).astype(BF16)


def decay_block(ctx_total, lat_total):
    row = lax.broadcasted_iota(jnp.int32, (8, 1), 0)
    block = jnp.zeros((8, 128), F32)
    for k, total in enumerate((ctx_total, lat_total)):
        hi, lo = split_hi_lo(total)
        block = jnp.where(row == 2 * k, hi, jnp.where(row == 2 * k + 1, lo, block))
    return block.astype(BF16)


def wide(v):
    heads = v.shape[1] // 2
    v = v.reshape(v.shape[0], 2, heads).transpose(0, 2, 1)
    return jnp.repeat(v, HEAD_DIM, axis=2).reshape(v.shape[0], heads * 2 * HEAD_DIM)


def twice(x):
    heads = x.shape[1] // HEAD_DIM
    v = x.reshape(x.shape[0], heads, 1, HEAD_DIM)
    return jnp.broadcast_to(v, (x.shape[0], heads, 2, HEAD_DIM)).reshape(x.shape[0], heads * 2 * HEAD_DIM)


def running_sums(log_decay):
    length = log_decay.shape[0]
    heads = log_decay.shape[1] // 2
    i = jnp.arange(length)
    low = (i[:, None] >= i[None, :]).astype(F32)
    forward = jnp.dot(low, log_decay[:, :heads], precision=HIGHEST)
    backward = jnp.dot(low.T, log_decay[:, heads:], precision=HIGHEST)
    return jnp.concatenate([forward, backward], axis=1)


def end_states(xs, bmat, dt, running, total):
    weights = wide(jnp.exp(total - running) * dt)
    weighted = (twice(xs).astype(F32) * weights).astype(BF16)
    return lax.dot_general(bmat, weighted, (((0,), (0,)), ((), ())), preferred_element_type=F32)


def entry_sums(states, totals, f_lane):
    n = states.shape[0]
    m = lax.broadcasted_iota(jnp.int32, (n + 1, n, n, 1), 0)
    k = lax.broadcasted_iota(jnp.int32, (n + 1, n, n, 1), 1)
    j = lax.broadcasted_iota(jnp.int32, (n + 1, n, n, 1), 2)
    mb = jnp.where(m == n, -1, m)
    between = jnp.where(f_lane, (j > k) & (j < m), (j < k) & (j > mb))
    gap = jnp.sum(jnp.where(between, totals[None, None], 0.0), axis=2)
    ahead = jnp.where(f_lane, k[:, :, 0] < m[:, :, 0], k[:, :, 0] > mb[:, :, 0])
    factor = jnp.where(ahead, jnp.exp(gap), 0.0)
    sums = jnp.sum(factor[:, :, None] * states[None], axis=1)
    to_m = jnp.sum(jnp.where(ahead, totals[None], 0.0), axis=1)
    return sums, to_m


def entry_states(ctx_state, ctx_total, lat_state, lat_total):
    heads = ctx_total.shape[1] // 2
    n = lax.axis_size(NEAR)
    half = heads * STATE // n

    def pieces(state):
        v = state.reshape(STATE // half, half, heads, 128).transpose(2, 0, 1, 3)
        return v.reshape(n, half, 128)

    block = decay_block(
        *(jnp.repeat(wide(t).reshape(heads, 1, 128), STATE // half, axis=0) for t in (ctx_total, lat_total))
    )
    near = jnp.concatenate([pieces(ctx_state).astype(BF16), pieces(lat_state).astype(BF16), block], axis=1)
    near = exchange(near, NEAR).astype(F32)
    f_lane = lax.broadcasted_iota(jnp.int32, (1, 128), 1) < HEAD_DIM
    ctx_t = near[:, 2 * half] + near[:, 2 * half + 1]
    lat_t = near[:, 2 * half + 2] + near[:, 2 * half + 3]
    ctx_sums, ctx_to = entry_sums(near[:, :half], ctx_t, f_lane)
    lat_sums, lat_to = entry_sums(near[:, half : 2 * half], lat_t, f_lane)
    far = jnp.concatenate(
        [ctx_sums[n].astype(BF16), lat_sums[n].astype(BF16), decay_block(ctx_to[n:], lat_to[n:])], axis=0
    )
    far = share(far, "za").astype(F32)
    count = far.shape[0]
    start, _ = entry_sums(far[:, :half], far[:, 2 * half] + far[:, 2 * half + 1], f_lane)
    group, group_to = entry_sums(far[:, half : 2 * half], far[:, 2 * half + 2] + far[:, 2 * half + 3], f_lane)
    mine = (jnp.arange(count + 1) == lax.axis_index("za")).astype(F32)
    group = jnp.sum(mine[:, None, None] * group, axis=0)
    group_to = jnp.sum(mine[:, None] * group_to, axis=0)
    entry = jnp.exp(group_to) * start[count] + group
    back = (jnp.exp(lat_to[:n, None]) * entry + lat_sums[:n]).astype(BF16)
    back = exchange(back, NEAR)
    return back.reshape(heads, STATE, 128)


def program(
    latent,
    cond,
    context,
    context_cond,
    modulation,
    norm_gain,
    w_x,
    w_gate,
    w_b,
    w_c,
    w_dt,
    conv_x,
    conv_b,
    conv_c,
    decay_rate,
    decay_extra,
    out_gain,
    w_out,
):
    heads = w_dt.shape[2]
    head_cols = w_x.shape[1]
    tokens = decay_extra.shape[0]
    ctx_tokens = context.shape[0]
    count = lax.axis_size(SP)
    place = lax.axis_index(SP)
    up = [(i, i + 1) for i in range(count - 1)]
    down = [(i + 1, i) for i in range(count - 1)]
    low = lax.ppermute(jnp.concatenate([latent[-PAD:], context[-PAD:]]), SP, up)
    high = lax.ppermute(jnp.concatenate([latent[:PAD], context[:PAD]]), SP, down)
    upper = lax.broadcasted_iota(jnp.int32, (PAD, 1), 0) < PAD // 2
    own = jnp.concatenate([latent, jnp.where(upper, high[:PAD], low[:PAD])])
    context_rows = jnp.concatenate([low[PAD:], context, high[PAD:]])
    held = (conv_x, conv_b, conv_c, decay_rate, decay_extra, norm_gain, w_dt, out_gain)
    mods, gathered, held = mod_vectors(cond, context_cond, modulation, own, held)
    conv_x, conv_b, conv_c, decay_rate, decay_extra, norm_gain, w_dt, out_gain = held
    tokens_own = latent.shape[0]
    latent_rows = jnp.concatenate(
        [
            gathered[-1, tokens_own:],
            gathered[:, :tokens_own].reshape(tokens, latent.shape[1]),
            gathered[0, tokens_own:],
        ]
    )

    lat_len = tokens + 2 * PAD
    hidden = jnp.concatenate(
        [
            modulated_norm(latent_rows, norm_gain, mods[0], mods[1]),
            modulated_norm(context_rows, norm_gain, mods[3], mods[4]),
        ]
    )
    row = jnp.arange(hidden.shape[0])
    first = (row < PAD) | ((row >= lat_len) & (row < lat_len + PAD))
    last = ((row >= lat_len - PAD) & (row < lat_len)) | (row >= hidden.shape[0] - PAD)
    outside = (first & (place == 0)) | (last & (place == count - 1))
    inner = hidden[PAD : PAD + tokens]

    def project(rows, weight):
        return jnp.dot(rows, weight, preferred_element_type=F32).astype(BF16)

    p_x = jnp.where(outside[:, None], 0.0, project(hidden, w_x).astype(F32))
    p_b = jnp.where(outside[:, None], 0.0, project(hidden, w_b).astype(F32))
    p_c = jnp.where(outside[:lat_len, None], 0.0, project(hidden[:lat_len], w_c).astype(F32))
    p_dt = jax.nn.softplus(project(hidden, jnp.concatenate([w_dt[0], w_dt[1]], axis=1)).astype(F32))
    z = project(inner, w_gate).astype(F32)

    off = PAD - 2
    xs = conv(p_x, conv_x, off, tokens)
    bmat = conv(p_b, conv_b, off, tokens)
    cmat = conv(p_c, conv_c, off, tokens)
    ctx_xs = conv(p_x, conv_x, lat_len + off, ctx_tokens)
    ctx_b = conv(p_b, conv_b, lat_len + off, ctx_tokens)
    dt = p_dt[PAD : PAD + tokens]
    ctx_dt = p_dt[lat_len + PAD : lat_len + PAD + ctx_tokens]
    rate = decay_rate.reshape(1, 2 * heads)
    log_decay = -rate * dt + jnp.concatenate([decay_extra, decay_extra], axis=1)
    ctx_log_decay = -rate * ctx_dt
    running = running_sums(log_decay)
    ctx_running = running_sums(ctx_log_decay)
    total = jnp.sum(log_decay, axis=0, keepdims=True)
    ctx_total = jnp.sum(ctx_log_decay, axis=0, keepdims=True)
    entry = entry_states(
        end_states(ctx_xs, ctx_b, ctx_dt, ctx_running, ctx_total),
        ctx_total,
        end_states(xs, bmat, dt, running, total),
        total,
    )

    affinity = lax.dot_general(cmat, bmat, (((1,), (1,)), ((), ())), preferred_element_type=F32)
    i = jnp.arange(tokens)
    lower = i[:, None] >= i[None, :]
    upper = i[:, None] <= i[None, :]
    parts = []
    for h in range(heads):
        weights = jnp.zeros((tokens, tokens), F32)
        for d, mask in ((0, lower), (1, upper)):
            col = d * heads + h
            gap = running[:, col][:, None] - running[:, col][None, :]
            mixing = jnp.where(mask, jnp.exp(jnp.where(mask, gap, 0.0)), 0.0)
            weights = weights + mixing * dt[:, col][None, :]
        weights = (affinity * weights).astype(BF16)
        parts.append(jnp.dot(weights, xs[:, h * HEAD_DIM : (h + 1) * HEAD_DIM], preferred_element_type=F32))
    y = jnp.concatenate(parts, axis=1)
    for d in range(2):
        flat = entry[:, :, d * HEAD_DIM : (d + 1) * HEAD_DIM].transpose(1, 0, 2).reshape(STATE, heads * HEAD_DIM)
        decayed = jnp.repeat(jnp.exp(running[:, d * heads : (d + 1) * heads]), HEAD_DIM, axis=1)
        y = y + jnp.dot(cmat, flat, preferred_element_type=F32) * decayed
    gated = y * jax.nn.silu(z)
    mean_square = jnp.mean(gated * gated, axis=1, keepdims=True)
    normed = (gated * lax.rsqrt(mean_square + GROUP_EPS) * out_gain.astype(F32)).astype(BF16)
    tp_count = lax.axis_size("tp")
    stacked = normed.reshape(tp_count, tokens // tp_count, head_cols)
    full = lax.all_to_all(stacked, "tp", split_axis=0, concat_axis=2, tiled=True)[0]
    branch = jnp.dot(full, w_out, preferred_element_type=F32)
    return (latent.astype(F32) + mods[2] * branch).astype(BF16)


def solution(mesh):
    sp, tp, dp = (mesh.shape[a] for a in ("sp", "tp", "dp"))
    inner = Mesh(np.asarray(mesh.devices).reshape(sp // 8, 4, 2, tp, dp), (*SP, "tp", "dp"))
    in_specs = (
        P(("dp", *SP, "tp"), None),
        P("dp"),
        P(("dp", *SP), None),
        P(),
        P((*SP, "tp"), None),
        P(),
        P(None, "tp"),
        P(None, "tp"),
        P(None, "tp"),
        P(None, "tp"),
        P(None, None, "tp"),
        P(None, "tp"),
        P(None, "tp"),
        P(None, "tp"),
        P(None, "tp"),
        P(("dp", *SP), "tp"),
        P("tp"),
        P(),
    )
    out_specs = P(("dp", *SP, "tp"), None)
    return jax.shard_map(program, mesh=inner, in_specs=in_specs, out_specs=out_specs, check_vma=False)
```

```python
import jax
import jax.numpy as jnp
import numpy as np
from jax import lax
from jax.experimental import pallas as pl
from jax.experimental.pallas import tpu as pltpu
from jax.sharding import Mesh
from jax.sharding import PartitionSpec as P


HEAD_DIM = 64
STATE = 64
ROW_EPS = 1e-06
GROUP_EPS = 1e-05
HIGHEST = lax.Precision.HIGHEST
F32 = jnp.float32
BF16 = jnp.bfloat16
PAD = 8

SP = ("za", "zb", "zc")
NEAR = ("zb", "zc")
MOD_NEAR = ("zc", "tp")
MOD_FAR = ("za", "zb")


def exchange(x, axis):
    return lax.all_to_all(x, axis, 0, 0, tiled=True)


def share(x, axis):
    n = lax.axis_size(axis)
    full = jnp.broadcast_to(x[None], (n, *x.shape)).reshape(n * x.shape[0], *x.shape[1:])
    return exchange(full, axis).reshape(n, *x.shape)


def ring_rows(x):
    n = lax.axis_size("tp")
    moved = [x] + [lax.ppermute(x, "tp", [(i, (i + k) % n) for i in range(n)]) for k in range(1, n)]
    moved = jnp.stack(moved)
    place = lax.axis_index("tp")
    return jnp.stack([lax.dynamic_index_in_dim(moved, (place - t) % n, 0, False) for t in range(n)])


def split_hi_lo(x):
    hi = lax.reduce_precision(x, 8, 7)
    return hi, x - hi


def whole(shape):
    return pl.BlockSpec(shape, lambda i: (0,) * len(shape))


def silu(v):
    return v / (1.0 + jnp.exp(-v))


def partial_kernel(first, cond, context_cond, modulation, out):
    share_rows, cols = modulation.shape
    width = cols // 3
    at = first[0] + lax.broadcasted_iota(jnp.int32, (share_rows, width), 0)
    pick = jnp.where(lax.broadcasted_iota(jnp.int32, (share_rows, width), 1) == at, 1.0, 0.0).astype(BF16)
    table = modulation[...]
    cut = width // (out.shape[0] // 5)
    for source, kinds in ((0, (0, 1, 2)), (1, (0, 1))):
        v = (cond, context_cond)[source][...].astype(F32).reshape(1, width)
        row = silu(v).astype(BF16)
        own = lax.dot_general(row, pick, (((1,), (1,)), ((), ())), preferred_element_type=F32).astype(BF16)
        sums = jnp.dot(own, table, preferred_element_type=F32)
        for kind in kinds:
            for n in range(width // cut):
                for r in range(2):
                    at = kind * width + n * cut + r * 128
                    out[n * 5 + 3 * source + kind, r : r + 1, :] = sums[0:1, at : at + 128]


def partial_mods(first, cond, context_cond, modulation, n):
    return pl.pallas_call(
        partial_kernel,
        grid=(1,),
        out_shape=jax.ShapeDtypeStruct((n * 5, 2, 128), F32),
        in_specs=[pl.BlockSpec(memory_space=pltpu.SMEM)] + [whole(v.shape) for v in (cond, context_cond, modulation)],
        out_specs=whole((n * 5, 2, 128)),
        name="partial_mods",
    )(first.astype(jnp.int32).reshape(1), cond, context_cond, modulation)


def mod_vectors(cond, context_cond, modulation, own_rows, held):
    share_rows = modulation.shape[0]
    width = modulation.shape[1] // 3
    n = lax.axis_size(MOD_NEAR)
    cut = width // n
    pairs = 5 * cut // 256
    first = lax.axis_index((*SP, "tp")) * share_rows
    part = partial_mods(first, cond, context_cond, modulation, n)
    part = jnp.sum(exchange(part, MOD_NEAR).reshape(n, pairs, 2, 128), axis=0)
    part, held = lax.optimization_barrier((part, held))
    far = share(part, MOD_FAR)
    gathered = ring_rows(own_rows)
    full = share(jnp.sum(far, axis=0), MOD_NEAR)
    return full.reshape(n, 5, cut).transpose(1, 0, 2).reshape(5, width), gathered, held


def modulated_norm(rows, norm_gain, shift_row, scale_row):
    values = rows.astype(F32)
    normed = values * lax.rsqrt(jnp.mean(values * values, axis=-1, keepdims=True) + ROW_EPS)
    return (normed * norm_gain.astype(F32) * (1.0 + scale_row) + shift_row).astype(BF16)


def conv(values, taps, first, length):
    total = jnp.zeros((length, values.shape[1]), F32)
    for k in range(4):
        total = total + taps[k].astype(F32) * values[first + k : first + k + length]
    return jax.nn.silu(total).astype(BF16)


def decay_block(ctx_total, lat_total):
    row = lax.broadcasted_iota(jnp.int32, (8, 1), 0)
    block = jnp.zeros((8, 128), F32)
    for k, total in enumerate((ctx_total, lat_total)):
        hi, lo = split_hi_lo(total)
        block = jnp.where(row == 2 * k, hi, jnp.where(row == 2 * k + 1, lo, block))
    return block.astype(BF16)


def wide(v):
    heads = v.shape[1] // 2
    v = v.reshape(v.shape[0], 2, heads).transpose(0, 2, 1)
    return jnp.repeat(v, HEAD_DIM, axis=2).reshape(v.shape[0], heads * 2 * HEAD_DIM)


def twice(x):
    heads = x.shape[1] // HEAD_DIM
    v = x.reshape(x.shape[0], heads, 1, HEAD_DIM)
    return jnp.broadcast_to(v, (x.shape[0], heads, 2, HEAD_DIM)).reshape(x.shape[0], heads * 2 * HEAD_DIM)


def running_sums(log_decay):
    length = log_decay.shape[0]
    heads = log_decay.shape[1] // 2
    i = jnp.arange(length)
    low = (i[:, None] >= i[None, :]).astype(F32)
    forward = jnp.dot(low, log_decay[:, :heads], precision=HIGHEST)
    backward = jnp.dot(low.T, log_decay[:, heads:], precision=HIGHEST)
    return jnp.concatenate([forward, backward], axis=1)


def end_states(xs, bmat, dt, running, total):
    weights = wide(jnp.exp(total - running) * dt)
    weighted = (twice(xs).astype(F32) * weights).astype(BF16)
    return lax.dot_general(bmat, weighted, (((0,), (0,)), ((), ())), preferred_element_type=F32)


def entry_sums(states, totals, f_lane):
    n = states.shape[0]
    m = lax.broadcasted_iota(jnp.int32, (n + 1, n, n, 1), 0)
    k = lax.broadcasted_iota(jnp.int32, (n + 1, n, n, 1), 1)
    j = lax.broadcasted_iota(jnp.int32, (n + 1, n, n, 1), 2)
    mb = jnp.where(m == n, -1, m)
    between = jnp.where(f_lane, (j > k) & (j < m), (j < k) & (j > mb))
    gap = jnp.sum(jnp.where(between, totals[None, None], 0.0), axis=2)
    ahead = jnp.where(f_lane, k[:, :, 0] < m[:, :, 0], k[:, :, 0] > mb[:, :, 0])
    factor = jnp.where(ahead, jnp.exp(gap), 0.0)
    sums = jnp.sum(factor[:, :, None] * states[None], axis=1)
    to_m = jnp.sum(jnp.where(ahead, totals[None], 0.0), axis=1)
    return sums, to_m


def entry_states(ctx_state, ctx_total, lat_state, lat_total):
    heads = ctx_total.shape[1] // 2
    n = lax.axis_size(NEAR)
    half = heads * STATE // n

    def pieces(state):
        v = state.reshape(STATE // half, half, heads, 128).transpose(2, 0, 1, 3)
        return v.reshape(n, half, 128)

    block = decay_block(
        *(jnp.repeat(wide(t).reshape(heads, 1, 128), STATE // half, axis=0) for t in (ctx_total, lat_total))
    )
    near = jnp.concatenate([pieces(ctx_state).astype(BF16), pieces(lat_state).astype(BF16), block], axis=1)
    near = exchange(near, NEAR).astype(F32)
    f_lane = lax.broadcasted_iota(jnp.int32, (1, 128), 1) < HEAD_DIM
    ctx_t = near[:, 2 * half] + near[:, 2 * half + 1]
    lat_t = near[:, 2 * half + 2] + near[:, 2 * half + 3]
    ctx_sums, ctx_to = entry_sums(near[:, :half], ctx_t, f_lane)
    lat_sums, lat_to = entry_sums(near[:, half : 2 * half], lat_t, f_lane)
    far = jnp.concatenate(
        [ctx_sums[n].astype(BF16), lat_sums[n].astype(BF16), decay_block(ctx_to[n:], lat_to[n:])], axis=0
    )
    far = share(far, "za").astype(F32)
    count = far.shape[0]
    start, _ = entry_sums(far[:, :half], far[:, 2 * half] + far[:, 2 * half + 1], f_lane)
    group, group_to = entry_sums(far[:, half : 2 * half], far[:, 2 * half + 2] + far[:, 2 * half + 3], f_lane)
    mine = (jnp.arange(count + 1) == lax.axis_index("za")).astype(F32)
    group = jnp.sum(mine[:, None, None] * group, axis=0)
    group_to = jnp.sum(mine[:, None] * group_to, axis=0)
    entry = jnp.exp(group_to) * start[count] + group
    back = (jnp.exp(lat_to[:n, None]) * entry + lat_sums[:n]).astype(BF16)
    back = exchange(back, NEAR)
    return back.reshape(heads, STATE, 128)


def program(
    latent,
    cond,
    context,
    context_cond,
    modulation,
    norm_gain,
    w_x,
    w_gate,
    w_b,
    w_c,
    w_dt,
    conv_x,
    conv_b,
    conv_c,
    decay_rate,
    decay_extra,
    out_gain,
    w_out,
):
    heads = w_dt.shape[2]
    head_cols = w_x.shape[1]
    tokens = decay_extra.shape[0]
    ctx_tokens = context.shape[0]
    count = lax.axis_size(SP)
    place = lax.axis_index(SP)
    up = [(i, i + 1) for i in range(count - 1)]
    down = [(i + 1, i) for i in range(count - 1)]
    low = lax.ppermute(jnp.concatenate([latent[-PAD:], context[-PAD:]]), SP, up)
    high = lax.ppermute(jnp.concatenate([latent[:PAD], context[:PAD]]), SP, down)
    upper = lax.broadcasted_iota(jnp.int32, (PAD, 1), 0) < PAD // 2
    own = jnp.concatenate([latent, jnp.where(upper, high[:PAD], low[:PAD])])
    context_rows = jnp.concatenate([low[PAD:], context, high[PAD:]])
    held = (conv_x, conv_b, conv_c, decay_rate, decay_extra, norm_gain, w_dt, out_gain)
    mods, gathered, held = mod_vectors(cond, context_cond, modulation, own, held)
    conv_x, conv_b, conv_c, decay_rate, decay_extra, norm_gain, w_dt, out_gain = held
    tokens_own = latent.shape[0]
    latent_rows = jnp.concatenate(
        [
            gathered[-1, tokens_own:],
            gathered[:, :tokens_own].reshape(tokens, latent.shape[1]),
            gathered[0, tokens_own:],
        ]
    )

    lat_len = tokens + 2 * PAD
    hidden = jnp.concatenate(
        [
            modulated_norm(latent_rows, norm_gain, mods[0], mods[1]),
            modulated_norm(context_rows, norm_gain, mods[3], mods[4]),
        ]
    )
    row = jnp.arange(hidden.shape[0])
    first = (row < PAD) | ((row >= lat_len) & (row < lat_len + PAD))
    last = ((row >= lat_len - PAD) & (row < lat_len)) | (row >= hidden.shape[0] - PAD)
    outside = (first & (place == 0)) | (last & (place == count - 1))
    inner = hidden[PAD : PAD + tokens]

    def project(rows, weight):
        return jnp.dot(rows, weight, preferred_element_type=F32).astype(BF16)

    p_x = jnp.where(outside[:, None], 0.0, project(hidden, w_x).astype(F32))
    p_b = jnp.where(outside[:, None], 0.0, project(hidden, w_b).astype(F32))
    p_c = jnp.where(outside[:lat_len, None], 0.0, project(hidden[:lat_len], w_c).astype(F32))
    p_dt = jax.nn.softplus(project(hidden, jnp.concatenate([w_dt[0], w_dt[1]], axis=1)).astype(F32))
    z = project(inner, w_gate).astype(F32)

    off = PAD - 2
    xs = conv(p_x, conv_x, off, tokens)
    bmat = conv(p_b, conv_b, off, tokens)
    cmat = conv(p_c, conv_c, off, tokens)
    ctx_xs = conv(p_x, conv_x, lat_len + off, ctx_tokens)
    ctx_b = conv(p_b, conv_b, lat_len + off, ctx_tokens)
    dt = p_dt[PAD : PAD + tokens]
    ctx_dt = p_dt[lat_len + PAD : lat_len + PAD + ctx_tokens]
    rate = decay_rate.reshape(1, 2 * heads)
    log_decay = -rate * dt + jnp.concatenate([decay_extra, decay_extra], axis=1)
    ctx_log_decay = -rate * ctx_dt
    running = running_sums(log_decay)
    ctx_running = running_sums(ctx_log_decay)
    total = jnp.sum(log_decay, axis=0, keepdims=True)
    ctx_total = jnp.sum(ctx_log_decay, axis=0, keepdims=True)
    entry = entry_states(
        end_states(ctx_xs, ctx_b, ctx_dt, ctx_running, ctx_total),
        ctx_total,
        end_states(xs, bmat, dt, running, total),
        total,
    )

    cmat, w_early = lax.optimization_barrier((cmat, w_out[: w_out.shape[0] // 4]))
    affinity = lax.dot_general(cmat, bmat, (((1,), (1,)), ((), ())), preferred_element_type=F32)
    i = jnp.arange(tokens)
    lower = i[:, None] >= i[None, :]
    upper = i[:, None] <= i[None, :]
    parts = []
    for h in range(heads):
        weights = jnp.zeros((tokens, tokens), F32)
        for d, mask in ((0, lower), (1, upper)):
            col = d * heads + h
            gap = running[:, col][:, None] - running[:, col][None, :]
            mixing = jnp.where(mask, jnp.exp(jnp.where(mask, gap, 0.0)), 0.0)
            weights = weights + mixing * dt[:, col][None, :]
        weights = (affinity * weights).astype(BF16)
        parts.append(jnp.dot(weights, xs[:, h * HEAD_DIM : (h + 1) * HEAD_DIM], preferred_element_type=F32))
    y = jnp.concatenate(parts, axis=1)
    for d in range(2):
        flat = entry[:, :, d * HEAD_DIM : (d + 1) * HEAD_DIM].transpose(1, 0, 2).reshape(STATE, heads * HEAD_DIM)
        decayed = jnp.repeat(jnp.exp(running[:, d * heads : (d + 1) * heads]), HEAD_DIM, axis=1)
        y = y + jnp.dot(cmat, flat, preferred_element_type=F32) * decayed
    gated = y * jax.nn.silu(z)
    mean_square = jnp.mean(gated * gated, axis=1, keepdims=True)
    normed = (gated * lax.rsqrt(mean_square + GROUP_EPS) * out_gain.astype(F32)).astype(BF16)
    tp_count = lax.axis_size("tp")
    stacked = normed.reshape(tp_count, tokens // tp_count, head_cols)
    full = lax.all_to_all(stacked, "tp", split_axis=0, concat_axis=2, tiled=True)[0]
    cut = w_early.shape[0]
    branch = jnp.dot(full[:, :cut], w_early, preferred_element_type=F32)
    branch = branch + jnp.dot(full[:, cut:], w_out[cut:], preferred_element_type=F32)
    return (latent.astype(F32) + mods[2] * branch).astype(BF16)


def solution(mesh):
    sp, tp, dp = (mesh.shape[a] for a in ("sp", "tp", "dp"))
    inner = Mesh(np.asarray(mesh.devices).reshape(sp // 8, 4, 2, tp, dp), (*SP, "tp", "dp"))
    in_specs = (
        P(("dp", *SP, "tp"), None),
        P("dp"),
        P(("dp", *SP), None),
        P(),
        P((*SP, "tp"), None),
        P(),
        P(None, "tp"),
        P(None, "tp"),
        P(None, "tp"),
        P(None, "tp"),
        P(None, None, "tp"),
        P(None, "tp"),
        P(None, "tp"),
        P(None, "tp"),
        P(None, "tp"),
        P(("dp", *SP), "tp"),
        P("tp"),
        P(),
    )
    out_specs = P(("dp", *SP, "tp"), None)
    return jax.shard_map(program, mesh=inner, in_specs=in_specs, out_specs=out_specs, check_vma=False)
```
